32 devices in a mesh: ep: 8 (over z, x), tp: 4 (over y, core).
Axes of the slice: x: 2, y: 2, z: 4, core: 2. Of those that a mesh axis runs over, the one named last changes fastest.
Arguments:
- queries: bfloat16 [2048, 1024], P('ep', 'tp'), may hold values from -6 to 6
- keys: bfloat16 [2048, 256], P('ep', 'tp'), may hold values from -6 to 6
- values: bfloat16 [2048, 256], P('ep', 'tp'), may hold values from -6 to 6
- q_gain: float32 [64], replicated, may hold values from 1 to 6
- k_gain: float32 [64], replicated, may hold values from 1 to 6
- out_weight: bfloat16 [1024, 2048], P('tp'), may hold values from -0.1875 to 0.1875
- tokens: bfloat16 [1024, 2048], P(('ep', 'tp')), may hold values from -6 to 6
- ffn_gain: float32 [2048], replicated, may hold values from 0.1 to 1.9
- route: int32 [1024, 2], P(('ep', 'tp')), may hold values from 0 to 7, all different within a row; in each aligned block of 32 rows (0 to 31, 32 to 63, ...) at most 16 rows name the same one
- route_weight: float32 [1024, 2], P(('ep', 'tp')), may hold values from 0.1 to 1
- gate_weight: bfloat16 [8, 2048, 3584], P('ep', None, 'tp'), may hold values from -0.125 to 0.125
- up_weight: bfloat16 [8, 2048, 3584], P('ep', None, 'tp'), may hold values from -0.125 to 0.125
- down_weight: bfloat16 [8, 3584, 2048], P('ep', 'tp'), may hold values from -0.09375 to 0.09375
Outputs:
- mixer_out: bfloat16 [2048, 2048], P(('ep', 'tp'))
- mixed: bfloat16 [1024, 2048], P(('ep', 'tp'))
The draws below stay inside these ranges and needn't reach their ends.
Inputs may be any that keep to these rules, and one draw needn't show every extreme that they name: `route`: each row names 2 different experts. In every device's aligned block of 32 rows no expert is named more than 16 times, and in some blocks some expert is named exactly 16 times.
All inputs are finite; a program needn't handle non-finite values.
Results may differ from the reference program's by a relative error of at most 0.013.
The reference program's roundings to bfloat16 on the way count: a program that leaves them out, or rounds other values in their place, can miss the bound.
Values may be sent and summed in bfloat16 or wider, within the bound.
A program may use at most 192 MiB of HBM per device.

```python
import math
import jax
import jax.numpy as jnp
import numpy as np
from jax import lax

D = 2048
HEADS = 16
KV_HEADS = 4
HEAD_DIM = 64
FF = 3584
TOPK = 2
GRID_W = 64
TOKENS_A = 2048
TOKENS_B = 1024
EXPERTS = 8
ROUTE_ROWS = 32
CAPACITY = 16
QW = 1024
KVW = 256
N_TP = 4


def draw_gain(key, salt):
    inner = jax.random.fold_in(key, salt)
    logs = jax.random.uniform(inner, (HEAD_DIM,), jnp.float32, 0.0, math.log(2.5))
    return jnp.exp(logs)


def draw_q_gain(key, part):
    return draw_gain(key, 21)


def draw_k_gain(key, part):
    return draw_gain(key, 22)


def draw_pair(key):
    query_key = jax.random.fold_in(key, 41)
    key_key = jax.random.fold_in(key, 42)
    query_vals = jnp.clip(jax.random.normal(query_key, (TOKENS_A, HEADS, HEAD_DIM), jnp.float32), -6.0, 6.0)
    key_vals = jnp.clip(jax.random.normal(key_key, (TOKENS_A, KV_HEADS, HEAD_DIM), jnp.float32), -6.0, 6.0)
    return (query_vals.reshape(TOKENS_A, HEADS * HEAD_DIM), key_vals.reshape(TOKENS_A, KV_HEADS * HEAD_DIM))


def draw_queries(key, part):
    return draw_pair(key)[0].astype(jnp.bfloat16)


def draw_keys(key, part):
    return draw_pair(key)[1].astype(jnp.bfloat16)


def block_levels(own_key, extent, shards, smallest, top_value):
    loudness = 1.0
    for position, blocks in shards:
        heights = jax.random.uniform(jax.random.fold_in(jax.random.fold_in(own_key, 6), position), (blocks,), jnp.float32, smallest / len(shards), top_value / len(shards))
        loudness = loudness * jnp.repeat(jnp.exp(heights), extent[position] // blocks).reshape((-1,) + (1,) * (len(extent) - 1 - position))
    return loudness


def assign_block(stream_key, own, number, rows, amount, top, reach, skew):
    order = jax.random.permutation(stream_key, amount)
    crowded, usual = portions_of(amount, rows * top, reach, skew, True), portions_of(amount, rows * top, reach, skew, False)
    places = jnp.arange(amount)

    def named(sizes, turn):
        used = int((sizes > 0).sum())
        fixed = max(1, used // 4)
        passed = fixed + (places - fixed + turn * (used - fixed)) % max(1, amount - fixed)
        return jnp.zeros((amount,), jnp.int32).at[order[jnp.where(places < fixed, places, passed)]].set(jnp.asarray(sizes, jnp.int32))

    sizes = jnp.where(number % 4 == 0, named(crowded, number // 4), named(usual, number - number // 4 - 1))
    mixed = jax.random.permutation(jax.random.fold_in(own, 3), amount)
    source_of, sink = mixed[0:amount // 2 * 2:2], mixed[1:amount // 2 * 2:2]
    slack = jnp.minimum(sizes[source_of] - 1, reach - sizes[sink]) // 2
    slack = jnp.where((source_of == order[0]) | (sink == order[0]) | (sizes[sink] == 0), 0, jnp.maximum(slack, 0))
    passed = jax.random.randint(jax.random.fold_in(own, 4), (amount // 2,), 0, 1 << 20) % (slack + 1)
    sizes = sizes.at[source_of].add(-passed).at[sink].add(passed)
    items = jnp.searchsorted(jnp.cumsum(sizes), jnp.arange(rows * top), side="right").astype(jnp.int32)
    grid = items.reshape(top, rows).T
    grid = grid[jax.random.permutation(jax.random.fold_in(own, 1), rows)]
    turn = jax.random.randint(jax.random.fold_in(own, 2), (rows, 1), 0, top)
    return jnp.take_along_axis(grid, (jnp.arange(top)[None, :] + turn) % top, axis=1)


def portions_of(number_of, total, reach, slope, full):
    portions = [(1 << 20) // math.isqrt(rank ** slope) + 1 for rank in range(1, number_of + 1)]
    largest = reach if full else min(reach, max(-(-total // number_of), total * portions[0] // sum(portions)))
    least = 1 if total - largest >= number_of - 1 else 0
    counts, surplus = [largest] + [least] * (number_of - 1), total - largest - least * (number_of - 1)
    while surplus > 0:
        movable = [i for i in range(1, number_of) if counts[i] < largest] or [i for i in range(1, number_of) if counts[i] < reach]
        mass, remaining = sum([portions[i] for i in movable]), surplus
        for i in movable:
            addition = min(reach - counts[i], max(1, remaining * portions[i] // mass), surplus)
            counts[i] = counts[i] + addition
            surplus = surplus - addition
    return np.array(counts)


def normal_values(own_key, extent, scale, most, cuts=(), kind=jnp.bfloat16):
    entries = scale * jax.random.normal(own_key, extent, jnp.float32)
    if cuts:
        entries = entries * block_levels(own_key, extent, cuts, -0.22, 0.18)
    return jnp.clip(entries, -most, most).astype(kind)


def setup_inputs(seed: int = 0) -> dict:
    splits = jax.random.split(jax.random.key(seed), 14)
    queries = draw_queries(jax.random.fold_in(splits[13], 71), 0)
    keys = draw_keys(jax.random.fold_in(splits[13], 71), 0)
    values = normal_values(splits[2], (TOKENS_A, KVW), 1.0, 6.0, ((0, 8), (1, 4)))
    q_gain = draw_q_gain(jax.random.fold_in(splits[13], 71), 0)
    k_gain = draw_k_gain(jax.random.fold_in(splits[13], 71), 0)
    out_weight = normal_values(splits[5], (QW, D), QW ** -0.5, 0.1875, ((0, 4),))
    tokens = normal_values(splits[6], (TOKENS_B, D), 1.0, 6.0, ((0, 32),))
    ffn_gain = jnp.clip(1.0 + 0.18 * jax.random.normal(splits[7], (D,), jnp.float32), 0.1, 1.9)
    route_keys = jax.random.split(jax.random.fold_in(splits[8], 1), TOKENS_B // ROUTE_ROWS)
    route_turns = jax.random.permutation(jax.random.fold_in(splits[8], 3), TOKENS_B // ROUTE_ROWS)
    route = jax.vmap(lambda own, number: assign_block(jax.random.fold_in(splits[8], 2), own, number, ROUTE_ROWS, EXPERTS, TOPK, CAPACITY, 1))(route_keys, route_turns).reshape((TOKENS_B, TOPK))
    route_weight = jnp.clip(0.1 + 0.9 * jax.random.uniform(splits[9], (TOKENS_B, TOPK), jnp.float32) ** block_levels(splits[9], (TOKENS_B, TOPK), ((0, 32),), -0.2, 0.2), 0.1, 1.0)
    gate_weight = normal_values(splits[10], (EXPERTS, D, FF), D ** -0.5, 0.125, ((0, 8), (2, 4)))
    up_weight = normal_values(splits[11], (EXPERTS, D, FF), D ** -0.5, 0.125, ((0, 8), (2, 4)))
    down_weight = normal_values(splits[12], (EXPERTS, FF, D), FF ** -0.5, 0.09375, ((0, 8), (1, 4)))
    return dict(queries=queries, keys=keys, values=values, q_gain=q_gain, k_gain=k_gain, out_weight=out_weight, tokens=tokens, ffn_gain=ffn_gain, route=route, route_weight=route_weight, gate_weight=gate_weight, up_weight=up_weight, down_weight=down_weight)


EPS = 1e-06
THETA = 10000.0

def head_norm(vals, gain):
    vals = vals.astype(jnp.float32)
    return vals * lax.rsqrt(lax.optimization_barrier(jnp.mean(vals * vals, axis=-1, keepdims=True)) + EPS) * gain

def rotate(vals, positions):
    pairs = vals.shape[-1] // 2
    quarter = pairs // 2
    freqs = THETA ** (-jnp.arange(quarter, dtype=jnp.float32) / quarter)
    grid_row = (positions // GRID_W).astype(jnp.float32)
    grid_col = (positions % GRID_W).astype(jnp.float32)
    angle = jnp.concatenate([grid_row[:, None] * freqs, grid_col[:, None] * freqs], axis=-1)
    cosine = jnp.cos(angle)[:, None, :]
    sine = jnp.sin(angle)[:, None, :]
    split = vals.reshape(vals.shape[:-1] + (pairs, 2))
    first = split[..., 0]
    second = split[..., 1]
    turned = jnp.stack([first * cosine - second * sine, first * sine + second * cosine], axis=-1)
    return turned.reshape(vals.shape)

def reference(queries, keys, values, q_gain, k_gain, out_weight, tokens, ffn_gain, route, route_weight, gate_weight, up_weight, down_weight):
    total = queries.shape[0]
    group = HEADS // KV_HEADS
    positions = jnp.arange(total, dtype=jnp.int32)
    rot_q = rotate(head_norm(queries.reshape(total, HEADS, HEAD_DIM), q_gain), positions).astype(jnp.bfloat16)
    rot_k = rotate(head_norm(keys.reshape(total, KV_HEADS, HEAD_DIM), k_gain), positions).astype(jnp.bfloat16)
    key_float = rot_k.astype(jnp.float32)
    value_float = values.reshape(total, KV_HEADS, HEAD_DIM).astype(jnp.float32)
    scale = HEAD_DIM ** (-0.5)
    block = math.gcd(total, 256)

    def attend(query_block):
        scores = jnp.einsum('qkgd,skd->qkgs', query_block.astype(jnp.float32), key_float) * scale
        highest = lax.optimization_barrier(jnp.max(scores, axis=-1, keepdims=True))
        expo = jnp.exp(scores - highest)
        denom = lax.optimization_barrier(jnp.sum(expo, axis=-1))
        probs = lax.optimization_barrier(expo.astype(jnp.bfloat16)).astype(jnp.float32)
        numer = jnp.einsum('qkgs,skd->qkgd', probs, value_float)
        return (numer / denom[..., None]).astype(jnp.bfloat16)
    query_blocks = rot_q.reshape(total // block, block, KV_HEADS, group, HEAD_DIM)
    attended = lax.map(attend, query_blocks).reshape(total, QW)
    share = QW // N_TP
    summed = jnp.zeros((total, D), jnp.float32)
    for index in range(N_TP):
        part = jnp.dot(attended[:, index * share:(index + 1) * share], out_weight[index * share:(index + 1) * share], preferred_element_type=jnp.float32)
        summed = summed + part.astype(jnp.bfloat16).astype(jnp.float32)
    mixer_out = summed.astype(jnp.bfloat16)
    token_float = tokens.astype(jnp.float32)
    normed = (token_float * lax.rsqrt(lax.optimization_barrier(jnp.mean(token_float * token_float, axis=-1, keepdims=True)) + EPS) * ffn_gain).astype(jnp.bfloat16)
    picks = route.reshape(-1)
    count = picks.shape[0]
    limit = tokens.shape[0] // ROUTE_ROWS * CAPACITY
    hidden_share = FF // N_TP

    def one_expert(expert):
        order = jnp.argsort((picks != expert).astype(jnp.int32), stable=True)[:limit].astype(jnp.int32)
        valid = picks[order] == expert
        chosen = normed[order // TOPK]
        gate = jnp.dot(chosen, gate_weight[expert], preferred_element_type=jnp.float32)
        upper = jnp.dot(chosen, up_weight[expert], preferred_element_type=jnp.float32)
        hidden = (jax.nn.silu(gate) * upper).astype(jnp.bfloat16)
        down = down_weight[expert]
        result = jnp.zeros((limit, D), jnp.float32)
        for index in range(N_TP):
            part = jnp.dot(hidden[:, index * hidden_share:(index + 1) * hidden_share], down[index * hidden_share:(index + 1) * hidden_share], preferred_element_type=jnp.float32)
            result = result + part.astype(jnp.bfloat16).astype(jnp.float32)
        target = jnp.where(valid, order, count).astype(jnp.int32)
        return (result.astype(jnp.bfloat16), target)
    outputs, targets = lax.map(one_expert, jnp.arange(EXPERTS, dtype=jnp.int32))
    per_pick = jnp.zeros((count, D), jnp.bfloat16).at[targets.reshape(-1)].set(outputs.reshape(-1, D), mode='drop')
    weighted = route_weight[..., None] * per_pick.reshape(tokens.shape[0], TOPK, D).astype(jnp.float32)
    mixed = lax.optimization_barrier(jnp.sum(weighted, axis=1)).astype(jnp.bfloat16)
    return (mixer_out, mixed)
```

```python
import functools
import math

import jax
import jax.numpy as jnp
from jax import lax
from jax.experimental import pallas as pl
from jax.experimental.pallas import tpu as pltpu
from jax.sharding import PartitionSpec as P

GRID_W = 64


EPS = 1e-06
THETA = 10000.0


def head_norm(vals, gain):
    vals = vals.astype(jnp.float32)
    return vals * lax.rsqrt(jnp.mean(vals * vals, axis=-1, keepdims=True) + EPS) * gain


def rotate(vals, positions):
    pairs = vals.shape[-1] // 2
    quarter = pairs // 2
    freqs = THETA ** (-jnp.arange(quarter, dtype=jnp.float32) / quarter)
    grid_row = (positions // GRID_W).astype(jnp.float32)
    grid_col = (positions % GRID_W).astype(jnp.float32)
    angle = jnp.concatenate([grid_row[:, None] * freqs, grid_col[:, None] * freqs], axis=-1)
    cosine = jnp.cos(angle)[:, None, :]
    sine = jnp.sin(angle)[:, None, :]
    split = vals.reshape(vals.shape[:-1] + (pairs, 2))
    first = split[..., 0]
    second = split[..., 1]
    turned = jnp.stack([first * cosine - second * sine, first * sine + second * cosine], axis=-1)
    return turned.reshape(vals.shape)


def local(
    queries,
    keys,
    values,
    q_gain,
    k_gain,
    out_weight,
    tokens,
    ffn_gain,
    route,
    route_weight,
    gate_weight,
    up_weight,
    down_weight,
):
    local_rows = queries.shape[0]
    head_size = q_gain.shape[0]
    query_heads = queries.shape[1] // head_size
    key_heads = keys.shape[1] // head_size
    group = query_heads // key_heads
    key_width = key_heads * head_size
    positions = lax.axis_index("ep") * local_rows + jnp.arange(local_rows, dtype=jnp.int32)
    rot_q = rotate(
        head_norm(queries.reshape(local_rows, query_heads, head_size), q_gain), positions
    ).astype(jnp.bfloat16)
    rot_q = rot_q.reshape(local_rows, key_heads, group, head_size)
    rot_k = rotate(
        head_norm(keys.reshape(local_rows, key_heads, head_size), k_gain), positions
    ).astype(jnp.bfloat16)
    joined = jnp.concatenate([rot_k.reshape(local_rows, key_width), values], axis=1)
    scale = head_size ** (-0.5)

    def fold_block(carry, block):
        highest, denom, numer = carry
        key_block = block[:, :key_width].reshape(-1, key_heads, head_size)
        value_block = block[:, key_width:].reshape(-1, key_heads, head_size)
        scores = (
            jnp.einsum("qkgd,skd->qkgs", rot_q, key_block, preferred_element_type=jnp.float32)
            * scale
        )
        new_high = jnp.maximum(highest, jnp.max(scores, axis=-1))
        shrink = jnp.exp(highest - new_high)
        expo = jnp.exp(scores - new_high[..., None])
        denom = denom * shrink + jnp.sum(expo, axis=-1)
        numer = numer * shrink[..., None] + jnp.einsum(
            "qkgs,skd->qkgd",
            expo.astype(jnp.bfloat16),
            value_block,
            preferred_element_type=jnp.float32,
        )
        return ((new_high, denom, numer), None)

    start_high = jnp.full((local_rows, key_heads, group), -1e30, jnp.float32)
    start_denom = jnp.zeros((local_rows, key_heads, group), jnp.float32)
    start_numer = jnp.zeros((local_rows, key_heads, group, head_size), jnp.float32)
    carry = (start_high, start_denom, start_numer)
    piece = lax.all_gather(joined, "ep", axis=0, tiled=True)
    length = piece.shape[0]
    size = length
    while size > 2048 and size % 2 == 0:
        size = size // 2
    blocks = piece.reshape(length // size, size, piece.shape[1])
    carry, _ = lax.scan(fold_block, carry, blocks)
    highest, denom, numer = carry
    attended = (
        (numer / denom[..., None]).astype(jnp.bfloat16).reshape(local_rows, query_heads * head_size)
    )
    own_rows = tokens.shape[0]
    width = tokens.shape[1]
    picks_row = route.shape[1]
    experts = lax.axis_size("ep")
    capacity = 2 * own_rows * picks_row // experts
    token_float = tokens.astype(jnp.float32)
    normed = (
        token_float
        * lax.rsqrt(jnp.mean(token_float * token_float, axis=-1, keepdims=True) + EPS)
        * ffn_gain
    ).astype(jnp.bfloat16)
    flat_route = route.reshape(-1)
    expert_hot = (flat_route[:, None] == jnp.arange(experts, dtype=jnp.int32)[None, :]).astype(
        jnp.int32
    )
    earlier = jnp.cumsum(expert_hot, axis=0) - expert_hot
    rank = jnp.sum(earlier * expert_hot, axis=1)
    slot = flat_route * capacity + rank
    pick_hot = (slot[:, None] == jnp.arange(experts * capacity, dtype=jnp.int32)[None, :]).astype(
        jnp.bfloat16
    )
    row_hot = jnp.sum(pick_hot.reshape(own_rows, picks_row, experts * capacity), axis=1)
    outgoing = jnp.einsum("rs,rd->sd", row_hot, normed, preferred_element_type=jnp.float32).astype(
        jnp.bfloat16
    )
    outgoing = outgoing.reshape(experts, capacity, width)
    gate_local = gate_weight[0]
    up_local = up_weight[0]
    down_local = down_weight[0]
    arrived = lax.all_to_all(outgoing, "ep", split_axis=0, concat_axis=0, tiled=True)
    sources = arrived.shape[0]
    items = arrived.shape[1]
    slot_rows = arrived.reshape(sources * items, width)
    piece = lax.all_gather(slot_rows, "tp", axis=0, tiled=True)
    gate = jnp.dot(piece, gate_local, preferred_element_type=jnp.float32)
    upper = jnp.dot(piece, up_local, preferred_element_type=jnp.float32)
    hidden = (jax.nn.silu(gate) * upper).astype(jnp.bfloat16)
    worked = jnp.dot(hidden, down_local, preferred_element_type=jnp.float32).reshape(
        -1, items, width
    )
    head_partial = jnp.dot(attended, out_weight, preferred_element_type=jnp.float32)
    mixer_sum, expert_sum = (
        lax.psum_scatter(
            head_partial.astype(jnp.bfloat16), "tp", scatter_dimension=0, tiled=True
        ).astype(jnp.float32),
        lax.psum_scatter(worked.astype(jnp.bfloat16), "tp", scatter_dimension=0, tiled=True).astype(
            jnp.float32
        ),
    )
    mixer_out = mixer_sum.astype(jnp.bfloat16)
    home = expert_sum.astype(jnp.bfloat16)
    back = lax.all_to_all(home, "ep", split_axis=0, concat_axis=0, tiled=True)
    copies = jnp.dot(
        pick_hot, back.reshape(experts * capacity, width), preferred_element_type=jnp.float32
    )
    weighted = route_weight[..., None] * copies.reshape(own_rows, picks_row, width)
    mixed = jnp.sum(weighted, axis=1).astype(jnp.bfloat16)
    return (mixer_out, mixed)


def norm_rotate(vals, gain, cosine, sine):
    vals = vals * lax.rsqrt(jnp.mean(vals * vals, axis=-1, keepdims=True) + EPS) * gain
    size = vals.shape[-1]
    lane = lax.broadcasted_iota(jnp.int32, vals.shape, 1)
    up = jnp.concatenate([vals[:, 1:], vals[:, :1]], axis=1)
    down = jnp.concatenate([vals[:, size - 1 :], vals[:, : size - 1]], axis=1)
    swapped = jnp.where(lane % 2 == 0, up, down)
    return vals * cosine + swapped * sine


def fused_kernel(
    dims,
    q_ref,
    k_ref,
    v_ref,
    qg_ref,
    kg_ref,
    tok_ref,
    fg_ref,
    route_t_ref,
    rw_ref,
    gate_hbm,
    up_hbm,
    down_hbm,
    ow_hbm,
    mix_ref,
    out_ref,
    wgu,
    wd,
    wo,
    og,
    slots,
    hidden,
    part,
    rs1,
    half,
    rs2,
    home,
    back,
    kvs,
    qp,
    att,
    mpart,
    mrs1,
    mhalf,
    mrs2,
    w_sem,
    a2a_s,
    a2a_r,
    f1_s,
    f1_r,
    f2_s,
    f2_r,
    f3_s,
    f3_r,
    kva_s,
    kva_r,
    kvb_s,
    kvb_r,
    r1_s,
    r1_r,
    r2_s,
    r2_r,
    bk_s,
    bk_r,
    m1_s,
    m1_r,
    m2_s,
    m2_r,
):
    ep, tp, cap, groups, tile = dims
    f32, bf16 = jnp.float32, jnp.bfloat16
    per = ep // groups
    order = peer_order(ep)
    place = {mask: i for i, mask in enumerate(order)}
    e = lax.axis_index("ep")
    t = lax.axis_index("tp")
    t1 = t + 1 - 2 * (t % 2)
    t2 = (t + 2) % tp
    own_rows, width = tok_ref.shape
    head_size, rows = k_ref.shape
    heads = q_ref.shape[1] // head_size
    units = hidden.shape[1]
    lane_tile = wgu.shape[2] // 2
    half_ep = ep // 2

    def peer(mask):
        other, bit = e, 1
        while bit < ep:
            if mask & bit:
                other = other + bit * (1 - 2 * ((e // bit) % 2))
            bit *= 2
        return other

    def remote(src, dst, ssem, rsem, pe, pt):
        return pltpu.make_async_remote_copy(
            src_ref=src,
            dst_ref=dst,
            send_sem=ssem,
            recv_sem=rsem,
            device_id={"ep": pe, "tp": pt},
            device_id_type=pl.DeviceIdType.MESH,
        )

    barrier = pltpu.get_barrier_semaphore()
    peers = [(peer(mask), t) for mask in range(1, ep)] + [(e, t1), (e, t2)]
    for pe, pt in peers:
        pl.semaphore_signal(
            barrier, inc=1, device_id={"ep": pe, "tp": pt}, device_id_type=pl.DeviceIdType.MESH
        )

    weights = []
    for n in range(units // lane_tile):
        cols = pl.ds(n * lane_tile, lane_tile)
        weights.append(
            pltpu.make_async_copy(
                gate_hbm.at[0, :, cols], wgu.at[n, :, pl.ds(0, lane_tile)], w_sem.at[2 * n]
            )
        )
        weights.append(
            pltpu.make_async_copy(
                up_hbm.at[0, :, cols],
                wgu.at[n, :, pl.ds(lane_tile, lane_tile)],
                w_sem.at[2 * n + 1],
            )
        )
    last = 2 * (units // lane_tile)
    weights.append(pltpu.make_async_copy(down_hbm.at[0], wd, w_sem.at[last]))
    load_out = pltpu.make_async_copy(ow_hbm, wo, w_sem.at[last + 1])
    for copy in weights:
        copy.start()
    load_out.start()

    slot_rows = ep * cap
    later = lax.broadcasted_iota(jnp.int32, (own_rows, own_rows), 0)
    early = lax.broadcasted_iota(jnp.int32, (own_rows, own_rows), 1)
    picks = []
    sends = jnp.zeros((slot_rows, own_rows), f32)
    topk = route_t_ref.shape[0]
    diag = later == early

    def column(row):
        return jnp.sum(jnp.where(diag, row, jnp.zeros_like(row)), axis=1, keepdims=True)

    def position_of(expert):
        spot = jnp.zeros_like(expert)
        for mask in range(ep):
            spot += jnp.where(expert == peer(mask), place[mask], 0)
        return spot

    columns = [column(route_t_ref[k : k + 1, :]) for k in range(topk)]
    for k in range(topk):
        col = columns[k]
        row = route_t_ref[k : k + 1, :]
        rank_col = jnp.zeros((own_rows, 1), f32)
        rank_row = jnp.zeros((1, own_rows), f32)
        for other in range(topk):
            same = (col == route_t_ref[other : other + 1, :]) & (early < later)
            rank_col += jnp.sum(jnp.where(same, 1.0, 0.0), axis=1, keepdims=True)
            same_t = (columns[other] == row) & (later < early)
            rank_row += jnp.sum(jnp.where(same_t, 1.0, 0.0), axis=0, keepdims=True)
        slot_col = (position_of(col) * cap).astype(f32) + rank_col
        slot_row = (position_of(row) * cap).astype(f32) + rank_row
        lanes = lax.broadcasted_iota(jnp.int32, (own_rows, slot_rows), 1).astype(f32)
        picks.append(jnp.where(lanes == slot_col, 1.0, 0.0).astype(bf16))
        subs = lax.broadcasted_iota(jnp.int32, (slot_rows, own_rows), 0).astype(f32)
        sends += jnp.where(subs == slot_row, 1.0, 0.0)
    tok = tok_ref[...].astype(f32)
    normed = (
        tok * lax.rsqrt(jnp.mean(tok * tok, axis=-1, keepdims=True) + EPS) * fg_ref[...]
    ).astype(bf16)
    outgoing = (
        jnp.dot(sends.astype(bf16), normed, preferred_element_type=f32)
        .astype(bf16)
        .reshape(ep, cap, width)
    )
    og[...] = outgoing
    slots[place[0] // per, 0, place[0] % per] = outgoing[place[0]]

    with jax.named_scope("barrier"):
        pl.semaphore_wait(barrier, len(peers))

    a2a, f1, f2, f3 = {}, {}, {}, {}
    for i in range(ep):
        g, m = i // per, i % per
        if order[i]:
            a2a[i] = remote(
                og.at[i], slots.at[g, 0, m], a2a_s.at[i], a2a_r.at[i], peer(order[i]), t
            )
        f1[i] = remote(slots.at[g, 0, m], slots.at[g, 1, m], f1_s.at[i], f1_r.at[i], e, t1)
        f2[i] = remote(slots.at[g, 0, m], slots.at[g, 2, m], f2_s.at[i], f2_r.at[i], e, t2)
        f3[i] = remote(slots.at[g, 2, m], slots.at[g, 3, m], f3_s.at[i], f3_r.at[i], e, t1)
    kva, kvb = {}, {}
    for k in range(half_ep):
        kvb[k] = remote(kvs.at[0, k], kvs.at[1, k], kvb_s.at[k], kvb_r.at[k], peer(1), t)
        if k:
            kva[k] = remote(
                kvs.at[0, 0], kvs.at[0, k], kva_s.at[k], kva_r.at[k], peer(2 * k), t
            )

    near, far = issue_order(ep)
    for mask in near:
        a2a[place[mask]].start()

    def forward(mask):
        i = place[mask]
        with jax.named_scope(f"fwd{mask}"):
            if mask:
                a2a[i].wait_recv()
            f2[i].start()
            f1[i].start()

    def relay(mask):
        i = place[mask]
        with jax.named_scope(f"relay{mask}"):
            f2[i].wait_recv()
            f3[i].start()

    forward(0)

    position = e * rows + lax.broadcasted_iota(jnp.int32, (rows, head_size), 0)
    channel = lax.broadcasted_iota(jnp.int32, (rows, head_size), 1)
    quarter = head_size // 4
    power = (channel // 2) % quarter
    freq = jnp.exp(power.astype(f32) * (-math.log(THETA) / quarter))
    grid_row = position // GRID_W
    spot = jnp.where(channel < head_size // 2, grid_row, position - grid_row * GRID_W)
    angle = spot.astype(f32) * freq
    cosine = jnp.cos(angle)
    sine = jnp.sin(angle) * jnp.where(channel % 2 == 0, -1.0, 1.0)
    both = jnp.concatenate([k_ref[...], v_ref[...]], axis=0).astype(f32).T
    rot_k = norm_rotate(both[:, :head_size], kg_ref[...], cosine, sine)
    kvs[0, 0, :, pl.ds(0, head_size)] = rot_k.astype(bf16)
    kvs[0, 0, :, pl.ds(head_size, head_size)] = both[:, head_size:].astype(bf16)

    for mask in far:
        a2a[place[mask]].start()
    for copy in kva.values():
        copy.start()
    kvb[0].start()

    for h in range(heads):
        lanes = pl.ds(h * head_size, head_size)
        turned = norm_rotate(q_ref[:, lanes].astype(f32), qg_ref[...], cosine, sine)
        qp[h, :, pl.ds(0, head_size)] = turned.astype(bf16)
        qp[h, :, pl.ds(head_size, head_size)] = jnp.zeros((rows, head_size), bf16)

    def share_keys(k):
        with jax.named_scope(f"share{k}"):
            kva[k].wait_recv()
            kvb[k].start()

    scale = head_size ** (-0.5) * math.log2(math.e)
    half_rows = rows // 2
    y = t // 2
    stack = 2

    def attend(side, h):
        start = pl.multiple_of(side * half_rows, half_rows)
        joined = kvs[...].reshape(ep * rows, 2 * head_size)
        chosen = qp[pl.ds(h, stack), pl.ds(start, half_rows), :]
        scores = lax.dot_general(
            chosen.reshape(stack * half_rows, 2 * head_size),
            joined,
            (((1,), (1,)), ((), ())),
            preferred_element_type=f32,
        )
        expo = jnp.exp2((scores - jnp.max(scores, axis=-1, keepdims=True)) * scale)
        denom = jnp.sum(expo, axis=-1, keepdims=True)
        numer = jnp.dot(expo.astype(bf16), joined, preferred_element_type=f32)
        result = (numer[:, head_size:] / denom).astype(bf16)
        for k in range(stack):
            att[pl.ds(start, half_rows), pl.ds((h + k) * head_size, head_size)] = result[
                k * half_rows : (k + 1) * half_rows
            ]

    mrows = rows // tp
    homes = [t, t1, t2, (t1 + 2) % tp]
    m1 = [
        remote(mpart.at[2 * i + 1], mrs1.at[i], m1_s.at[i], m1_r.at[i], e, t1) for i in range(2)
    ]
    m2 = remote(mhalf, mrs2, m2_s, m2_r, e, t2)

    def project(js):
        for j in js:
            piece = att[pl.ds(pl.multiple_of(homes[j] * mrows, mrows), mrows), :]
            mpart[j] = jnp.dot(piece, wo[...], preferred_element_type=f32).astype(bf16)
            if j % 2:
                m1[j // 2].start()

    def feed_wait(g):
        with jax.named_scope(f"feedwait{g}"):
            for i in range(g * per, (g + 1) * per):
                f1[i].wait_recv()
                f3[i].wait_recv()

    rows_g = tp * per * cap

    def up(g):
        with jax.named_scope(f"up{g}"):
            chosen = slots[g].reshape(rows_g, width)
            for n in range(units // lane_tile):
                both = jnp.dot(chosen, wgu[n], preferred_element_type=f32)
                gate = both[:, :lane_tile]
                act = gate / (1.0 + jnp.exp(-gate)) * both[:, lane_tile:]
                hidden[:, pl.ds(n * lane_tile, lane_tile)] = act.astype(bf16)

    def down(g):
        with jax.named_scope(f"down{g}"):
            for n in range(width // tile):
                cols = pl.ds(n * tile, tile)
                result = jnp.dot(hidden[...], wd[:, cols], preferred_element_type=f32)
                part[g, :, :, :, cols] = result.astype(bf16).reshape(tp, per, cap, tile)
        r1[g, 1].start()
        r1[g, 0].start()

    r1, r2 = {}, {}
    for g in range(groups):
        for i in range(2):
            r1[g, i] = remote(
                part.at[g, 2 * i + 1], rs1.at[g, i], r1_s.at[g, i], r1_r.at[g, i], e, t1
            )
        r2[g] = remote(half.at[g], rs2.at[g], r2_s.at[g], r2_r.at[g], e, t2)
    bk = {}
    for i in range(ep):
        if order[i]:
            bk[i] = remote(
                home.at[i // per, i % per], back.at[i], bk_s.at[i], bk_r.at[i], peer(order[i]), t
            )

    def pair_sum(g):
        with jax.named_scope(f"pairsum{g}"):
            r1[g, 1].wait_recv()
            half[g] = (part[g, 2].astype(f32) + rs1[g, 1].astype(f32)).astype(bf16)
            r2[g].start()

    def finish(g):
        with jax.named_scope(f"finish{g}"):
            r1[g, 0].wait_recv()
            r2[g].wait_recv()
            total = (
                part[g, 0].astype(f32) + rs1[g, 0].astype(f32) + rs2[g].astype(f32)
            ).astype(bf16)
            home[g] = total
            for i in range(g * per, (g + 1) * per):
                if order[i]:
                    bk[i].start()
                else:
                    back[i] = total[i % per]

    def mixer_half():
        with jax.named_scope("mixhalf"):
            m1[1].wait_recv()
            mhalf[...] = (mpart[2].astype(f32) + mrs1[1].astype(f32)).astype(bf16)
            m2.start()

    forward(1)
    forward(2)
    relay(0)
    relay(1)
    forward(3)
    forward(4)
    relay(2)
    for copy in weights:
        copy.wait()
    feed_wait(0)
    up(0)
    down(0)
    relay(3)
    forward(5)
    relay(4)
    forward(6)
    forward(7)
    feed_wait(1)
    share_keys(1)
    up(1)
    pair_sum(0)
    relay(5)
    down(1)
    relay(6)
    share_keys(2)
    feed_wait(2)
    up(2)
    relay(7)
    pair_sum(1)
    down(2)
    share_keys(3)
    feed_wait(3)
    up(3)
    pair_sum(2)
    down(3)
    finish(0)
    pair_sum(3)
    with jax.named_scope("kvwait"):
        for k in range(half_ep):
            kvb[k].wait_recv()
    with jax.named_scope("att0"):
        attend(1 - y, 0)
    finish(1)
    with jax.named_scope("att1"):
        attend(1 - y, 2)
    load_out.wait()
    with jax.named_scope("project"):
        project((3, 2))
    finish(2)
    with jax.named_scope("att2"):
        attend(y, 0)
    mixer_half()
    with jax.named_scope("att3"):
        attend(y, 2)
    finish(3)
    with jax.named_scope("project"):
        project((1, 0))
    with jax.named_scope("mwait"):
        m1[0].wait_recv()
        m2.wait_recv()
    mix_ref[...] = (
        mpart[0].astype(f32) + mrs1[0].astype(f32) + mrs2[...].astype(f32)
    ).astype(bf16)
    with jax.named_scope("bkwait"):
        for copy in bk.values():
            copy.wait_recv()
    returned = back[...].reshape(slot_rows, width)
    mixed = jnp.zeros((own_rows, width), f32)
    for k in range(topk):
        mixed += column(rw_ref[k : k + 1, :]) * jnp.dot(
            picks[k], returned, preferred_element_type=f32
        )
    out_ref[...] = mixed.astype(bf16)

    for group in (kva, kvb, a2a, f1, f2, f3, r1, r2, bk):
        for copy in group.values():
            copy.wait_send()
    for copy in m1 + [m2]:
        copy.wait_send()


def peer_order(ep):
    return tuple(range(1, ep)) + (0,)


def issue_order(ep):
    return tuple(range(1, ep)), ()


def store_kernel(mix_ref, rows_ref, mix_out, rows_out, sems):
    copies = [
        pltpu.make_async_copy(mix_ref, mix_out, sems.at[0]),
        pltpu.make_async_copy(rows_ref, rows_out, sems.at[1]),
    ]
    for copy in copies:
        copy.start()
    for copy in copies:
        copy.wait()


def local_fused(
    queries,
    keys,
    values,
    q_gain,
    k_gain,
    out_weight,
    tokens,
    ffn_gain,
    route,
    route_weight,
    gate_weight,
    up_weight,
    down_weight,
):
    ep = lax.axis_size("ep")
    tp = lax.axis_size("tp")
    rows = queries.shape[0]
    head_size = q_gain.shape[0]
    heads = queries.shape[1] // head_size
    own_rows, width = tokens.shape
    cap = 2 * own_rows * route.shape[1] // ep
    units = gate_weight.shape[2]
    lane_tile = 128
    tile = math.gcd(width, 512)
    groups = GROUPS
    per = ep // groups
    bf16 = jnp.bfloat16
    vmem = pl.BlockSpec(memory_space=pltpu.VMEM)
    hbm = pl.BlockSpec(memory_space=pl.ANY)
    dma = pltpu.SemaphoreType.DMA
    mrows = rows // tp
    flops = 2 * tp * ep * cap * width * units * 3 + 4 * heads * rows * rows * ep * head_size
    held = pl.pallas_call(
        functools.partial(fused_kernel, (ep, tp, cap, groups, tile)),
        out_shape=(
            pltpu.VMEM((mrows, width), bf16),
            pltpu.VMEM((own_rows, width), bf16),
        ),
        in_specs=[vmem] * 9 + [hbm] * 4,
        out_specs=(vmem, vmem),
        scratch_shapes=[
            pltpu.VMEM((units // lane_tile, width, 2 * lane_tile), bf16),
            pltpu.VMEM((units, width), bf16),
            pltpu.VMEM(out_weight.shape, bf16),
            pltpu.VMEM((ep, cap, width), bf16),
            pltpu.VMEM((groups, tp, per, cap, width), bf16),
            pltpu.VMEM((tp * per * cap, units), bf16),
            pltpu.VMEM((groups, tp, per, cap, width), bf16),
            pltpu.VMEM((groups, 2, per, cap, width), bf16),
            pltpu.VMEM((groups, per, cap, width), bf16),
            pltpu.VMEM((groups, per, cap, width), bf16),
            pltpu.VMEM((groups, per, cap, width), bf16),
            pltpu.VMEM((ep, cap, width), bf16),
            pltpu.VMEM((2, ep // 2, rows, 2 * head_size), bf16),
            pltpu.VMEM((heads, rows, 2 * head_size), bf16),
            pltpu.VMEM((rows, heads * head_size), bf16),
            pltpu.VMEM((tp, mrows, width), bf16),
            pltpu.VMEM((2, mrows, width), bf16),
            pltpu.VMEM((mrows, width), bf16),
            pltpu.VMEM((mrows, width), bf16),
            dma((2 * (units // lane_tile) + 2,)),
        ]
        + [dma((ep,))] * 8
        + [dma((ep // 2,))] * 4
        + [dma((groups, 2))] * 2
        + [dma((groups,))] * 2
        + [dma((ep,))] * 2
        + [dma((2,))] * 2
        + [dma, dma],
        compiler_params=pltpu.CompilerParams(
            collective_id=0, has_side_effects=True, vmem_limit_bytes=60 * 1024 * 1024
        ),
        cost_estimate=pl.CostEstimate(
            flops=flops, bytes_accessed=3 * 2 * width * units, transcendentals=0
        ),
    )(
        queries,
        keys.T,
        values.T,
        q_gain[None, :],
        k_gain[None, :],
        tokens,
        ffn_gain[None, :],
        route.T,
        route_weight.T,
        gate_weight,
        up_weight,
        down_weight,
        out_weight,
    )
    return pl.pallas_call(
        store_kernel,
        out_shape=tuple(jax.ShapeDtypeStruct(part.shape, bf16) for part in held),
        in_specs=[vmem] * len(held),
        out_specs=(hbm,) * len(held),
        scratch_shapes=[dma((len(held),))],
    )(*[pltpu.with_memory_space_constraint(part, pltpu.VMEM) for part in held])


GROUPS = 4


def step(*args):
    queries, keys, q_gain, tokens, route, gate_weight = (args[i] for i in (0, 1, 3, 6, 8, 10))
    ep, tp = lax.axis_size("ep"), lax.axis_size("tp")
    cap = 2 * tokens.shape[0] * route.shape[1] // ep
    fits = (
        tp == 4
        and ep == 8
        and queries.shape[1] % (2 * q_gain.shape[0]) == 0
        and ep % GROUPS == 0
        and cap % 16 == 0
        and keys.shape[1] == q_gain.shape[0]
        and gate_weight.shape[2] % 128 == 0
        and queries.shape[0] % (16 * tp) == 0
    )
    return local_fused(*args) if fits else local(*args)


def solution(mesh):
    placed = (
        P("ep", "tp"),
        P("ep", "tp"),
        P("ep", "tp"),
        P(),
        P(),
        P("tp", None),
        P(("ep", "tp"), None),
        P(),
        P(("ep", "tp"), None),
        P(("ep", "tp"), None),
        P("ep", None, "tp"),
        P("ep", None, "tp"),
        P("ep", "tp", None),
    )
    return jax.shard_map(
        step,
        mesh=mesh,
        in_specs=placed,
        out_specs=(P(("ep", "tp"), None), P(("ep", "tp"), None)),
        check_vma=False,
    )
```

```python
import functools
import math

import jax
import jax.numpy as jnp
from jax import lax
from jax.experimental import pallas as pl
from jax.experimental.pallas import tpu as pltpu
from jax.sharding import PartitionSpec as P

GRID_W = 64


EPS = 1e-06
THETA = 10000.0


def head_norm(vals, gain):
    vals = vals.astype(jnp.float32)
    return vals * lax.rsqrt(jnp.mean(vals * vals, axis=-1, keepdims=True) + EPS) * gain


def rotate(vals, positions):
    pairs = vals.shape[-1] // 2
    quarter = pairs // 2
    freqs = THETA ** (-jnp.arange(quarter, dtype=jnp.float32) / quarter)
    grid_row = (positions // GRID_W).astype(jnp.float32)
    grid_col = (positions % GRID_W).astype(jnp.float32)
    angle = jnp.concatenate([grid_row[:, None] * freqs, grid_col[:, None] * freqs], axis=-1)
    cosine = jnp.cos(angle)[:, None, :]
    sine = jnp.sin(angle)[:, None, :]
    split = vals.reshape(vals.shape[:-1] + (pairs, 2))
    first = split[..., 0]
    second = split[..., 1]
    turned = jnp.stack([first * cosine - second * sine, first * sine + second * cosine], axis=-1)
    return turned.reshape(vals.shape)


def local(
    queries,
    keys,
    values,
    q_gain,
    k_gain,
    out_weight,
    tokens,
    ffn_gain,
    route,
    route_weight,
    gate_weight,
    up_weight,
    down_weight,
):
    local_rows = queries.shape[0]
    head_size = q_gain.shape[0]
    query_heads = queries.shape[1] // head_size
    key_heads = keys.shape[1] // head_size
    group = query_heads // key_heads
    key_width = key_heads * head_size
    positions = lax.axis_index("ep") * local_rows + jnp.arange(local_rows, dtype=jnp.int32)
    rot_q = rotate(
        head_norm(queries.reshape(local_rows, query_heads, head_size), q_gain), positions
    ).astype(jnp.bfloat16)
    rot_q = rot_q.reshape(local_rows, key_heads, group, head_size)
    rot_k = rotate(
        head_norm(keys.reshape(local_rows, key_heads, head_size), k_gain), positions
    ).astype(jnp.bfloat16)
    joined = jnp.concatenate([rot_k.reshape(local_rows, key_width), values], axis=1)
    scale = head_size ** (-0.5)

    def fold_block(carry, block):
        highest, denom, numer = carry
        key_block = block[:, :key_width].reshape(-1, key_heads, head_size)
        value_block = block[:, key_width:].reshape(-1, key_heads, head_size)
        scores = (
            jnp.einsum("qkgd,skd->qkgs", rot_q, key_block, preferred_element_type=jnp.float32)
            * scale
        )
        new_high = jnp.maximum(highest, jnp.max(scores, axis=-1))
        shrink = jnp.exp(highest - new_high)
        expo = jnp.exp(scores - new_high[..., None])
        denom = denom * shrink + jnp.sum(expo, axis=-1)
        numer = numer * shrink[..., None] + jnp.einsum(
            "qkgs,skd->qkgd",
            expo.astype(jnp.bfloat16),
            value_block,
            preferred_element_type=jnp.float32,
        )
        return ((new_high, denom, numer), None)

    start_high = jnp.full((local_rows, key_heads, group), -1e30, jnp.float32)
    start_denom = jnp.zeros((local_rows, key_heads, group), jnp.float32)
    start_numer = jnp.zeros((local_rows, key_heads, group, head_size), jnp.float32)
    carry = (start_high, start_denom, start_numer)
    piece = lax.all_gather(joined, "ep", axis=0, tiled=True)
    length = piece.shape[0]
    size = length
    while size > 2048 and size % 2 == 0:
        size = size // 2
    blocks = piece.reshape(length // size, size, piece.shape[1])
    carry, _ = lax.scan(fold_block, carry, blocks)
    highest, denom, numer = carry
    attended = (
        (numer / denom[..., None]).astype(jnp.bfloat16).reshape(local_rows, query_heads * head_size)
    )
    own_rows = tokens.shape[0]
    width = tokens.shape[1]
    picks_row = route.shape[1]
    experts = lax.axis_size("ep")
    capacity = 2 * own_rows * picks_row // experts
    token_float = tokens.astype(jnp.float32)
    normed = (
        token_float
        * lax.rsqrt(jnp.mean(token_float * token_float, axis=-1, keepdims=True) + EPS)
        * ffn_gain
    ).astype(jnp.bfloat16)
    flat_route = route.reshape(-1)
    expert_hot = (flat_route[:, None] == jnp.arange(experts, dtype=jnp.int32)[None, :]).astype(
        jnp.int32
    )
    earlier = jnp.cumsum(expert_hot, axis=0) - expert_hot
    rank = jnp.sum(earlier * expert_hot, axis=1)
    slot = flat_route * capacity + rank
    pick_hot = (slot[:, None] == jnp.arange(experts * capacity, dtype=jnp.int32)[None, :]).astype(
        jnp.bfloat16
    )
    row_hot = jnp.sum(pick_hot.reshape(own_rows, picks_row, experts * capacity), axis=1)
    outgoing = jnp.einsum("rs,rd->sd", row_hot, normed, preferred_element_type=jnp.float32).astype(
        jnp.bfloat16
    )
    outgoing = outgoing.reshape(experts, capacity, width)
    gate_local = gate_weight[0]
    up_local = up_weight[0]
    down_local = down_weight[0]
    arrived = lax.all_to_all(outgoing, "ep", split_axis=0, concat_axis=0, tiled=True)
    sources = arrived.shape[0]
    items = arrived.shape[1]
    slot_rows = arrived.reshape(sources * items, width)
    piece = lax.all_gather(slot_rows, "tp", axis=0, tiled=True)
    gate = jnp.dot(piece, gate_local, preferred_element_type=jnp.float32)
    upper = jnp.dot(piece, up_local, preferred_element_type=jnp.float32)
    hidden = (jax.nn.silu(gate) * upper).astype(jnp.bfloat16)
    worked = jnp.dot(hidden, down_local, preferred_element_type=jnp.float32).reshape(
        -1, items, width
    )
    head_partial = jnp.dot(attended, out_weight, preferred_element_type=jnp.float32)
    mixer_sum, expert_sum = (
        lax.psum_scatter(
            head_partial.astype(jnp.bfloat16), "tp", scatter_dimension=0, tiled=True
        ).astype(jnp.float32),
        lax.psum_scatter(worked.astype(jnp.bfloat16), "tp", scatter_dimension=0, tiled=True).astype(
            jnp.float32
        ),
    )
    mixer_out = mixer_sum.astype(jnp.bfloat16)
    home = expert_sum.astype(jnp.bfloat16)
    back = lax.all_to_all(home, "ep", split_axis=0, concat_axis=0, tiled=True)
    copies = jnp.dot(
        pick_hot, back.reshape(experts * capacity, width), preferred_element_type=jnp.float32
    )
    weighted = route_weight[..., None] * copies.reshape(own_rows, picks_row, width)
    mixed = jnp.sum(weighted, axis=1).astype(jnp.bfloat16)
    return (mixer_out, mixed)


def norm_rotate(vals, gain, cosine, sine):
    vals = vals * lax.rsqrt(jnp.mean(vals * vals, axis=-1, keepdims=True) + EPS) * gain
    size = vals.shape[-1]
    lane = lax.broadcasted_iota(jnp.int32, vals.shape, 1)
    up = jnp.concatenate([vals[:, 1:], vals[:, :1]], axis=1)
    down = jnp.concatenate([vals[:, size - 1 :], vals[:, : size - 1]], axis=1)
    swapped = jnp.where(lane % 2 == 0, up, down)
    return vals * cosine + swapped * sine


def fused_kernel(
    dims,
    q_ref,
    k_ref,
    v_ref,
    qg_ref,
    kg_ref,
    tok_ref,
    fg_ref,
    route_t_ref,
    rw_ref,
    gate_hbm,
    up_hbm,
    down_hbm,
    ow_hbm,
    mix_ref,
    out_ref,
    wgu,
    wd,
    wo,
    og,
    slots,
    hidden,
    part,
    rs1,
    half,
    rs2,
    home,
    back,
    kvs,
    qp,
    att,
    mpart,
    mrs1,
    mhalf,
    mrs2,
    passing,
    w_sem,
    a2a_s,
    a2a_r,
    f1_s,
    f1_r,
    f2_s,
    f2_r,
    f3_s,
    f3_r,
    kva_s,
    kva_r,
    kvb_s,
    kvb_r,
    r1_s,
    r1_r,
    r2_s,
    r2_r,
    bk_s,
    bk_r,
    m1_s,
    m1_r,
    m2_s,
    m2_r,
    y2_s,
    y2_r,
):
    ep, tp, cap, groups, tile = dims
    f32, bf16 = jnp.float32, jnp.bfloat16
    per = ep // groups
    order = peer_order(ep)
    place = {mask: i for i, mask in enumerate(order)}
    e = lax.axis_index("ep")
    t = lax.axis_index("tp")
    t1 = t + 1 - 2 * (t % 2)
    t2 = (t + 2) % tp
    own_rows, width = tok_ref.shape
    head_size, rows = k_ref.shape
    heads = q_ref.shape[1] // head_size
    units = hidden.shape[1]
    lane_tile = wgu.shape[2] // 2
    half_ep = ep // 2

    def peer(mask):
        other, bit = e, 1
        while bit < ep:
            if mask & bit:
                other = other + bit * (1 - 2 * ((e // bit) % 2))
            bit *= 2
        return other

    def remote(src, dst, ssem, rsem, pe, pt):
        return pltpu.make_async_remote_copy(
            src_ref=src,
            dst_ref=dst,
            send_sem=ssem,
            recv_sem=rsem,
            device_id={"ep": pe, "tp": pt},
            device_id_type=pl.DeviceIdType.MESH,
        )

    def landed(ref, sem):
        pltpu.make_async_copy(ref, ref, sem).wait()

    barrier = pltpu.get_barrier_semaphore()
    peers = [(peer(mask), t) for mask in range(1, ep)] + [(e, t1), (e, t2)]
    for pe, pt in peers:
        pl.semaphore_signal(
            barrier, inc=1, device_id={"ep": pe, "tp": pt}, device_id_type=pl.DeviceIdType.MESH
        )

    for n in range(units // lane_tile):
        cols = pl.ds(n * lane_tile, lane_tile)
        for side, source in ((0, gate_hbm), (lane_tile, up_hbm)):
            pltpu.make_async_copy(
                source.at[0, :, cols], wgu.at[n, :, pl.ds(side, lane_tile)], w_sem.at[0]
            ).start()
    load_down = pltpu.make_async_copy(down_hbm.at[0], wd, w_sem.at[1])
    load_out = pltpu.make_async_copy(ow_hbm, wo, w_sem.at[2])
    load_down.start()
    load_out.start()

    slot_rows = ep * cap
    later = lax.broadcasted_iota(jnp.int32, (own_rows, own_rows), 0)
    early = lax.broadcasted_iota(jnp.int32, (own_rows, own_rows), 1)
    picks = []
    sends = jnp.zeros((slot_rows, own_rows), f32)
    topk = route_t_ref.shape[0]
    diag = later == early

    def column(row):
        return jnp.sum(jnp.where(diag, row, jnp.zeros_like(row)), axis=1, keepdims=True)

    def position_of(expert):
        spot = jnp.zeros_like(expert)
        for mask in range(ep):
            spot += jnp.where(expert == peer(mask), place[mask], 0)
        return spot

    mix_weights = [column(rw_ref[k : k + 1, :]) for k in range(topk)]
    columns = [column(route_t_ref[k : k + 1, :]) for k in range(topk)]
    for k in range(topk):
        col = columns[k]
        row = route_t_ref[k : k + 1, :]
        rank_col = jnp.zeros((own_rows, 1), f32)
        rank_row = jnp.zeros((1, own_rows), f32)
        for other in range(topk):
            same = (col == route_t_ref[other : other + 1, :]) & (early < later)
            rank_col += jnp.sum(jnp.where(same, 1.0, 0.0), axis=1, keepdims=True)
            same_t = (columns[other] == row) & (later < early)
            rank_row += jnp.sum(jnp.where(same_t, 1.0, 0.0), axis=0, keepdims=True)
        slot_col = (position_of(col) * cap).astype(f32) + rank_col
        slot_row = (position_of(row) * cap).astype(f32) + rank_row
        lanes = lax.broadcasted_iota(jnp.int32, (own_rows, slot_rows), 1).astype(f32)
        picks.append(jnp.where(lanes == slot_col, 1.0, 0.0).astype(bf16))
        subs = lax.broadcasted_iota(jnp.int32, (slot_rows, own_rows), 0).astype(f32)
        sends += jnp.where(subs == slot_row, 1.0, 0.0)
    tok = tok_ref[...].astype(f32)
    normed = (
        tok * lax.rsqrt(jnp.mean(tok * tok, axis=-1, keepdims=True) + EPS) * fg_ref[...]
    ).astype(bf16)
    outgoing = (
        jnp.dot(sends.astype(bf16), normed, preferred_element_type=f32)
        .astype(bf16)
        .reshape(ep, cap, width)
    )
    og[...] = outgoing
    slots[place[0] // per, 0, place[0] % per] = outgoing[place[0]]

    with jax.named_scope("barrier"):
        pl.semaphore_wait(barrier, len(peers))

    a2a, f1, f2, f3, y2 = {}, {}, {}, {}, {}
    for i in range(ep):
        g, m = i // per, i % per
        if order[i]:
            a2a[i] = remote(
                og.at[i], slots.at[g, 0, m], a2a_s, a2a_r.at[i], peer(order[i]), t
            )
        f1[i] = remote(slots.at[g, 0, m], slots.at[g, 1, m], f1_s, f1_r.at[g], e, t1)
        mask = order[i]
        if 0 < mask < half_ep:
            f2[i] = remote(og.at[i], passing.at[mask], f2_s, f2_r.at[i], e, t2)
            y2[i] = remote(
                passing.at[mask], slots.at[g, 2, m], y2_s, y2_r.at[mask], peer(mask), t
            )
        else:
            f2[i] = remote(slots.at[g, 0, m], slots.at[g, 2, m], f2_s, f2_r.at[i], e, t2)
        f3[i] = remote(slots.at[g, 2, m], slots.at[g, 3, m], f3_s, f3_r.at[g], e, t1)
    kva, kvb = {}, {}
    for k in range(half_ep):
        kvb[k] = remote(kvs.at[0, k], kvs.at[1, k], kvb_s, kvb_r, peer(1), t)
        if k in (1, 2):
            kva[k] = remote(
                kvs.at[0, 0], kvs.at[0, k], kva_s, kva_r.at[k], peer(2 * k), t
            )
        if k == 3:
            kva[k] = remote(
                kvs.at[0, 2], kvs.at[0, 3], kva_s, kva_r.at[k], peer(2), t
            )

    near, far = issue_order(ep)
    for mask in near:
        a2a[place[mask]].start()
    for mask in range(1, half_ep):
        f2[place[mask]].start()
    for mask in far:
        a2a[place[mask]].start()

    def forward(mask):
        i = place[mask]
        with jax.named_scope(f"fwd{mask}"):
            if mask:
                a2a[i].wait_recv()
            if not 0 < mask < half_ep:
                f2[i].start()
            f1[i].start()

    def pass_on(mask):
        i = place[mask]
        with jax.named_scope(f"pass{mask}"):
            f2[i].wait_recv()
            y2[i].start()

    def relay(mask):
        i = place[mask]
        with jax.named_scope(f"relay{mask}"):
            (y2[i] if 0 < mask < half_ep else f2[i]).wait_recv()
            f3[i].start()

    forward(0)

    position = e * rows + lax.broadcasted_iota(jnp.int32, (rows, head_size), 0)
    channel = lax.broadcasted_iota(jnp.int32, (rows, head_size), 1)
    quarter = head_size // 4
    power = (channel // 2) % quarter
    freq = jnp.exp(power.astype(f32) * (-math.log(THETA) / quarter))
    grid_row = position // GRID_W
    spot = jnp.where(channel < head_size // 2, grid_row, position - grid_row * GRID_W)
    angle = spot.astype(f32) * freq
    cosine = jnp.cos(angle)
    sine = jnp.sin(angle) * jnp.where(channel % 2 == 0, -1.0, 1.0)
    both = jnp.concatenate([k_ref[...], v_ref[...]], axis=0).astype(f32).T
    rot_k = norm_rotate(both[:, :head_size], kg_ref[...], cosine, sine)
    kvs[0, 0, :, pl.ds(0, head_size)] = rot_k.astype(bf16)
    kvs[0, 0, :, pl.ds(head_size, head_size)] = both[:, head_size:].astype(bf16)

    kvb[0].start()

    for h in range(heads):
        lanes = pl.ds(h * head_size, head_size)
        turned = norm_rotate(q_ref[:, lanes].astype(f32), qg_ref[...], cosine, sine)
        qp[h, :, pl.ds(0, head_size)] = turned.astype(bf16)
        qp[h, :, pl.ds(head_size, head_size)] = jnp.zeros((rows, head_size), bf16)

    def share_keys(k):
        with jax.named_scope(f"share{k}"):
            kva[k].wait_recv()
            if k == 2:
                kva[3].start()
            kvb[k].start()

    scale = head_size ** (-0.5) * math.log2(math.e)
    half_rows = rows // 2
    y = t // 2
    stack = 2

    def attend(side, h):
        start = pl.multiple_of(side * half_rows, half_rows)
        joined = kvs[...].reshape(ep * rows, 2 * head_size)
        chosen = qp[pl.ds(h, stack), pl.ds(start, half_rows), :]
        scores = lax.dot_general(
            chosen.reshape(stack * half_rows, 2 * head_size),
            joined,
            (((1,), (1,)), ((), ())),
            preferred_element_type=f32,
        )
        expo = jnp.exp2((scores - jnp.max(scores, axis=-1, keepdims=True)) * scale)
        denom = jnp.sum(expo, axis=-1, keepdims=True)
        numer = jnp.dot(expo.astype(bf16), joined, preferred_element_type=f32)
        result = (numer[:, head_size:] / denom).astype(bf16)
        for k in range(stack):
            att[pl.ds(start, half_rows), pl.ds((h + k) * head_size, head_size)] = result[
                k * half_rows : (k + 1) * half_rows
            ]

    mrows = rows // tp
    homes = [t, t1, t2, (t1 + 2) % tp]
    m1 = [
        remote(mpart.at[2 * i + 1], mrs1.at[i], m1_s, m1_r.at[i], e, t1) for i in range(2)
    ]
    m2 = remote(mhalf, mrs2, m2_s, m2_r, e, t2)

    def project(js):
        for j in js:
            piece = att[pl.ds(pl.multiple_of(homes[j] * mrows, mrows), mrows), :]
            mpart[j] = jnp.dot(piece, wo[...], preferred_element_type=f32).astype(bf16)
            if j % 2:
                m1[j // 2].start()

    def feed_wait(g):
        with jax.named_scope(f"feedwait{g}"):
            landed(slots.at[g, 1], f1_r.at[g])
            landed(slots.at[g, 3], f3_r.at[g])

    rows_g = tp * per * cap

    def up(g):
        with jax.named_scope(f"up{g}"):
            chosen = slots[g].reshape(rows_g, width)
            for n in range(units // lane_tile):
                both = jnp.dot(chosen, wgu[n], preferred_element_type=f32)
                gate = both[:, :lane_tile]
                act = gate / (1.0 + jnp.exp(-gate)) * both[:, lane_tile:]
                hidden[:, pl.ds(n * lane_tile, lane_tile)] = act.astype(bf16)

    def down(g):
        with jax.named_scope(f"down{g}"):
            for n in range(width // tile):
                cols = pl.ds(n * tile, tile)
                result = jnp.dot(hidden[...], wd[:, cols], preferred_element_type=f32)
                part[g, :, :, :, cols] = result.astype(bf16).reshape(tp, per, cap, tile)
        r1[g, 1].start()
        r1[g, 0].start()

    r1, r2 = {}, {}
    for g in range(groups):
        for i in range(2):
            r1[g, i] = remote(
                part.at[g, 2 * i + 1], rs1.at[g, i], r1_s, r1_r.at[g, i], e, t1
            )
        r2[g] = remote(half.at[g], rs2.at[g], r2_s, r2_r.at[g], e, t2)
    bk = {}
    for i in range(ep):
        if order[i]:
            bk[i] = remote(
                home.at[i // per, i % per], back.at[i], bk_s, bk_r, peer(order[i]), t
            )

    def pair_sum(g):
        with jax.named_scope(f"pairsum{g}"):
            r1[g, 1].wait_recv()
            half[g] = (part[g, 2].astype(f32) + rs1[g, 1].astype(f32)).astype(bf16)
            r2[g].start()

    def finish(g):
        with jax.named_scope(f"finish{g}"):
            r1[g, 0].wait_recv()
            r2[g].wait_recv()
            total = (
                part[g, 0].astype(f32) + rs1[g, 0].astype(f32) + rs2[g].astype(f32)
            ).astype(bf16)
            home[g] = total
            for i in range(g * per, (g + 1) * per):
                if order[i]:
                    bk[i].start()
                else:
                    back[i] = total[i % per]

    def mixer_half():
        with jax.named_scope("mixhalf"):
            m1[1].wait_recv()
            mhalf[...] = (mpart[2].astype(f32) + mrs1[1].astype(f32)).astype(bf16)
            m2.start()

    kva[2].start()
    pass_on(1)
    forward(1)
    pass_on(2)
    pass_on(3)
    kva[1].start()
    relay(1)
    forward(4)
    forward(2)
    forward(3)
    relay(0)
    pltpu.make_async_copy(wgu, wgu, w_sem.at[0]).wait()
    load_down.wait()
    relay(4)
    forward(5)
    feed_wait(0)
    up(0)
    relay(2)
    forward(6)
    down(0)
    forward(7)
    relay(5)
    feed_wait(1)
    share_keys(2)
    up(1)
    pair_sum(0)
    relay(3)
    relay(6)
    down(1)
    relay(7)
    share_keys(1)
    feed_wait(2)
    up(2)
    share_keys(3)
    pair_sum(1)
    down(2)
    feed_wait(3)
    up(3)
    finish(0)
    pair_sum(2)
    down(3)
    with jax.named_scope("kvwait"):
        landed(kvs.at[1], kvb_r)
    with jax.named_scope("att0"):
        attend(1 - y, 0)
    pair_sum(3)
    finish(1)
    with jax.named_scope("att1"):
        attend(1 - y, 2)
    load_out.wait()
    with jax.named_scope("project"):
        project((3, 2))
    with jax.named_scope("att2"):
        attend(y, 0)
    mixer_half()
    finish(2)
    with jax.named_scope("att3"):
        attend(y, 2)
    with jax.named_scope("project"):
        project((1, 0))
    finish(3)
    others = pl.ds(0, ep - 1)
    landed(og.at[others], a2a_s)
    for sem in (f1_s, f2_s, f3_s):
        landed(og, sem)
    landed(og.at[pl.ds(0, half_ep - 1)], y2_s)
    landed(kvs.at[0, pl.ds(0, half_ep - 1)], kva_s)
    landed(kvs.at[0], kvb_s)
    landed(rs1, r1_s)
    landed(rs2, r2_s)
    with jax.named_scope("bkwait"):
        landed(back.at[pl.ds(0, ep - 1)], bk_r)
    returned = back[...].reshape(slot_rows, width)
    chosen = jnp.dot(jnp.concatenate(picks, axis=0), returned, preferred_element_type=f32)
    mixed = jnp.zeros((own_rows, width), f32)
    for k in range(topk):
        mixed += mix_weights[k] * chosen[k * own_rows : (k + 1) * own_rows]
    out_ref[...] = mixed.astype(bf16)
    with jax.named_scope("mwait"):
        m1[0].wait_recv()
        m2.wait_recv()
    mix_ref[...] = (
        mpart[0].astype(f32) + mrs1[0].astype(f32) + mrs2[...].astype(f32)
    ).astype(bf16)
    landed(og.at[others], bk_s)
    landed(mrs1, m1_s)
    m2.wait_send()


def peer_order(ep):
    half = ep // 2
    near = tuple(range(1, half)) + (0,)
    return tuple(m for i, k in enumerate(near) for m in (k, half + i))


def issue_order(ep):
    return (1, 2, 3), tuple(range(4, ep))


def store_kernel(mix_ref, rows_ref, mix_out, rows_out, sems):
    copies = [
        pltpu.make_async_copy(mix_ref, mix_out, sems.at[0]),
        pltpu.make_async_copy(rows_ref, rows_out, sems.at[1]),
    ]
    for copy in copies:
        copy.start()
    for copy in copies:
        copy.wait()


def local_fused(
    queries,
    keys,
    values,
    q_gain,
    k_gain,
    out_weight,
    tokens,
    ffn_gain,
    route,
    route_weight,
    gate_weight,
    up_weight,
    down_weight,
):
    ep = lax.axis_size("ep")
    tp = lax.axis_size("tp")
    rows = queries.shape[0]
    head_size = q_gain.shape[0]
    heads = queries.shape[1] // head_size
    own_rows, width = tokens.shape
    cap = 2 * own_rows * route.shape[1] // ep
    units = gate_weight.shape[2]
    lane_tile = 128
    tile = math.gcd(width, 512)
    groups = GROUPS
    per = ep // groups
    bf16 = jnp.bfloat16
    vmem = pl.BlockSpec(memory_space=pltpu.VMEM)
    hbm = pl.BlockSpec(memory_space=pl.ANY)
    dma = pltpu.SemaphoreType.DMA
    mrows = rows // tp
    flops = 2 * tp * ep * cap * width * units * 3 + 4 * heads * rows * rows * ep * head_size
    held = pl.pallas_call(
        functools.partial(fused_kernel, (ep, tp, cap, groups, tile)),
        out_shape=(
            pltpu.VMEM((mrows, width), bf16),
            pltpu.VMEM((own_rows, width), bf16),
        ),
        in_specs=[vmem] * 9 + [hbm] * 4,
        out_specs=(vmem, vmem),
        scratch_shapes=[
            pltpu.VMEM((units // lane_tile, width, 2 * lane_tile), bf16),
            pltpu.VMEM((units, width), bf16),
            pltpu.VMEM(out_weight.shape, bf16),
            pltpu.VMEM((ep, cap, width), bf16),
            pltpu.VMEM((groups, tp, per, cap, width), bf16),
            pltpu.VMEM((tp * per * cap, units), bf16),
            pltpu.VMEM((groups, tp, per, cap, width), bf16),
            pltpu.VMEM((groups, 2, per, cap, width), bf16),
            pltpu.VMEM((groups, per, cap, width), bf16),
            pltpu.VMEM((groups, per, cap, width), bf16),
            pltpu.VMEM((groups, per, cap, width), bf16),
            pltpu.VMEM((ep, cap, width), bf16),
            pltpu.VMEM((2, ep // 2, rows, 2 * head_size), bf16),
            pltpu.VMEM((heads, rows, 2 * head_size), bf16),
            pltpu.VMEM((rows, heads * head_size), bf16),
            pltpu.VMEM((tp, mrows, width), bf16),
            pltpu.VMEM((2, mrows, width), bf16),
            pltpu.VMEM((mrows, width), bf16),
            pltpu.VMEM((mrows, width), bf16),
            pltpu.VMEM((ep // 2, cap, width), bf16),
            dma((3,)),
        ]
        + [dma, dma((ep,)), dma, dma((groups,)), dma, dma((ep,)), dma, dma((groups,))]
        + [dma, dma((ep // 2,)), dma, dma]
        + [dma, dma((groups, 2)), dma, dma((groups,)), dma, dma]
        + [dma, dma((2,)), dma, dma]
        + [dma, dma((ep // 2,))],
        compiler_params=pltpu.CompilerParams(
            collective_id=0, has_side_effects=True, vmem_limit_bytes=60 * 1024 * 1024
        ),
        cost_estimate=pl.CostEstimate(
            flops=flops, bytes_accessed=3 * 2 * width * units, transcendentals=0
        ),
    )(
        queries,
        keys.T,
        values.T,
        q_gain[None, :],
        k_gain[None, :],
        tokens,
        ffn_gain[None, :],
        route.T,
        route_weight.T,
        gate_weight,
        up_weight,
        down_weight,
        out_weight,
    )
    return pl.pallas_call(
        store_kernel,
        out_shape=tuple(jax.ShapeDtypeStruct(part.shape, bf16) for part in held),
        in_specs=[vmem] * len(held),
        out_specs=(hbm,) * len(held),
        scratch_shapes=[dma((len(held),))],
    )(*[pltpu.with_memory_space_constraint(part, pltpu.VMEM) for part in held])


GROUPS = 4


def step(*args):
    queries, keys, q_gain, tokens, route, gate_weight = (args[i] for i in (0, 1, 3, 6, 8, 10))
    ep, tp = lax.axis_size("ep"), lax.axis_size("tp")
    cap = 2 * tokens.shape[0] * route.shape[1] // ep
    fits = (
        tp == 4
        and ep == 8
        and queries.shape[1] % (2 * q_gain.shape[0]) == 0
        and ep % GROUPS == 0
        and cap % 16 == 0
        and keys.shape[1] == q_gain.shape[0]
        and gate_weight.shape[2] % 128 == 0
        and queries.shape[0] % (16 * tp) == 0
    )
    return local_fused(*args) if fits else local(*args)


def solution(mesh):
    placed = (
        P("ep", "tp"),
        P("ep", "tp"),
        P("ep", "tp"),
        P(),
        P(),
        P("tp", None),
        P(("ep", "tp"), None),
        P(),
        P(("ep", "tp"), None),
        P(("ep", "tp"), None),
        P("ep", None, "tp"),
        P("ep", None, "tp"),
        P("ep", "tp", None),
    )
    return jax.shard_map(
        step,
        mesh=mesh,
        in_specs=placed,
        out_specs=(P(("ep", "tp"), None), P(("ep", "tp"), None)),
        check_vma=False,
    )
```

```python
import functools
import math

import jax
import jax.numpy as jnp
from jax import lax
from jax.experimental import pallas as pl
from jax.experimental.pallas import tpu as pltpu
from jax.sharding import PartitionSpec as P

GRID_W = 64


EPS = 1e-06
THETA = 10000.0


def head_norm(vals, gain):
    vals = vals.astype(jnp.float32)
    return vals * lax.rsqrt(jnp.mean(vals * vals, axis=-1, keepdims=True) + EPS) * gain


def rotate(vals, positions):
    pairs = vals.shape[-1] // 2
    quarter = pairs // 2
    freqs = THETA ** (-jnp.arange(quarter, dtype=jnp.float32) / quarter)
    grid_row = (positions // GRID_W).astype(jnp.float32)
    grid_col = (positions % GRID_W).astype(jnp.float32)
    angle = jnp.concatenate([grid_row[:, None] * freqs, grid_col[:, None] * freqs], axis=-1)
    cosine = jnp.cos(angle)[:, None, :]
    sine = jnp.sin(angle)[:, None, :]
    split = vals.reshape(vals.shape[:-1] + (pairs, 2))
    first = split[..., 0]
    second = split[..., 1]
    turned = jnp.stack([first * cosine - second * sine, first * sine + second * cosine], axis=-1)
    return turned.reshape(vals.shape)


def local(
    queries,
    keys,
    values,
    q_gain,
    k_gain,
    out_weight,
    tokens,
    ffn_gain,
    route,
    route_weight,
    gate_weight,
    up_weight,
    down_weight,
):
    local_rows = queries.shape[0]
    head_size = q_gain.shape[0]
    query_heads = queries.shape[1] // head_size
    key_heads = keys.shape[1] // head_size
    group = query_heads // key_heads
    key_width = key_heads * head_size
    positions = lax.axis_index("ep") * local_rows + jnp.arange(local_rows, dtype=jnp.int32)
    rot_q = rotate(
        head_norm(queries.reshape(local_rows, query_heads, head_size), q_gain), positions
    ).astype(jnp.bfloat16)
    rot_q = rot_q.reshape(local_rows, key_heads, group, head_size)
    rot_k = rotate(
        head_norm(keys.reshape(local_rows, key_heads, head_size), k_gain), positions
    ).astype(jnp.bfloat16)
    joined = jnp.concatenate([rot_k.reshape(local_rows, key_width), values], axis=1)
    scale = head_size ** (-0.5)

    def fold_block(carry, block):
        highest, denom, numer = carry
        key_block = block[:, :key_width].reshape(-1, key_heads, head_size)
        value_block = block[:, key_width:].reshape(-1, key_heads, head_size)
        scores = (
            jnp.einsum("qkgd,skd->qkgs", rot_q, key_block, preferred_element_type=jnp.float32)
            * scale
        )
        new_high = jnp.maximum(highest, jnp.max(scores, axis=-1))
        shrink = jnp.exp(highest - new_high)
        expo = jnp.exp(scores - new_high[..., None])
        denom = denom * shrink + jnp.sum(expo, axis=-1)
        numer = numer * shrink[..., None] + jnp.einsum(
            "qkgs,skd->qkgd",
            expo.astype(jnp.bfloat16),
            value_block,
            preferred_element_type=jnp.float32,
        )
        return ((new_high, denom, numer), None)

    start_high = jnp.full((local_rows, key_heads, group), -1e30, jnp.float32)
    start_denom = jnp.zeros((local_rows, key_heads, group), jnp.float32)
    start_numer = jnp.zeros((local_rows, key_heads, group, head_size), jnp.float32)
    carry = (start_high, start_denom, start_numer)
    piece = lax.all_gather(joined, "ep", axis=0, tiled=True)
    length = piece.shape[0]
    size = length
    while size > 2048 and size % 2 == 0:
        size = size // 2
    blocks = piece.reshape(length // size, size, piece.shape[1])
    carry, _ = lax.scan(fold_block, carry, blocks)
    highest, denom, numer = carry
    attended = (
        (numer / denom[..., None]).astype(jnp.bfloat16).reshape(local_rows, query_heads * head_size)
    )
    own_rows = tokens.shape[0]
    width = tokens.shape[1]
    picks_row = route.shape[1]
    experts = lax.axis_size("ep")
    capacity = 2 * own_rows * picks_row // experts
    token_float = tokens.astype(jnp.float32)
    normed = (
        token_float
        * lax.rsqrt(jnp.mean(token_float * token_float, axis=-1, keepdims=True) + EPS)
        * ffn_gain
    ).astype(jnp.bfloat16)
    flat_route = route.reshape(-1)
    expert_hot = (flat_route[:, None] == jnp.arange(experts, dtype=jnp.int32)[None, :]).astype(
        jnp.int32
    )
    earlier = jnp.cumsum(expert_hot, axis=0) - expert_hot
    rank = jnp.sum(earlier * expert_hot, axis=1)
    slot = flat_route * capacity + rank
    pick_hot = (slot[:, None] == jnp.arange(experts * capacity, dtype=jnp.int32)[None, :]).astype(
        jnp.bfloat16
    )
    row_hot = jnp.sum(pick_hot.reshape(own_rows, picks_row, experts * capacity), axis=1)
    outgoing = jnp.einsum("rs,rd->sd", row_hot, normed, preferred_element_type=jnp.float32).astype(
        jnp.bfloat16
    )
    outgoing = outgoing.reshape(experts, capacity, width)
    gate_local = gate_weight[0]
    up_local = up_weight[0]
    down_local = down_weight[0]
    arrived = lax.all_to_all(outgoing, "ep", split_axis=0, concat_axis=0, tiled=True)
    sources = arrived.shape[0]
    items = arrived.shape[1]
    slot_rows = arrived.reshape(sources * items, width)
    piece = lax.all_gather(slot_rows, "tp", axis=0, tiled=True)
    gate = jnp.dot(piece, gate_local, preferred_element_type=jnp.float32)
    upper = jnp.dot(piece, up_local, preferred_element_type=jnp.float32)
    hidden = (jax.nn.silu(gate) * upper).astype(jnp.bfloat16)
    worked = jnp.dot(hidden, down_local, preferred_element_type=jnp.float32).reshape(
        -1, items, width
    )
    head_partial = jnp.dot(attended, out_weight, preferred_element_type=jnp.float32)
    mixer_sum, expert_sum = (
        lax.psum_scatter(
            head_partial.astype(jnp.bfloat16), "tp", scatter_dimension=0, tiled=True
        ).astype(jnp.float32),
        lax.psum_scatter(worked.astype(jnp.bfloat16), "tp", scatter_dimension=0, tiled=True).astype(
            jnp.float32
        ),
    )
    mixer_out = mixer_sum.astype(jnp.bfloat16)
    home = expert_sum.astype(jnp.bfloat16)
    back = lax.all_to_all(home, "ep", split_axis=0, concat_axis=0, tiled=True)
    copies = jnp.dot(
        pick_hot, back.reshape(experts * capacity, width), preferred_element_type=jnp.float32
    )
    weighted = route_weight[..., None] * copies.reshape(own_rows, picks_row, width)
    mixed = jnp.sum(weighted, axis=1).astype(jnp.bfloat16)
    return (mixer_out, mixed)


def norm_rotate(vals, gain, cosine, sine):
    vals = vals * lax.rsqrt(jnp.mean(vals * vals, axis=-1, keepdims=True) + EPS) * gain
    size = vals.shape[-1]
    lane = lax.broadcasted_iota(jnp.int32, vals.shape, 1)
    up = jnp.concatenate([vals[:, 1:], vals[:, :1]], axis=1)
    down = jnp.concatenate([vals[:, size - 1 :], vals[:, : size - 1]], axis=1)
    swapped = jnp.where(lane % 2 == 0, up, down)
    return vals * cosine + swapped * sine


def fused_kernel(
    dims,
    q_hbm,
    k_hbm,
    v_hbm,
    qg_hbm,
    kg_hbm,
    tok_hbm,
    fg_hbm,
    route_hbm,
    rw_hbm,
    gate_hbm,
    up_hbm,
    down_hbm,
    ow_hbm,
    mix_ref,
    out_ref,
    q_ref,
    k_ref,
    v_ref,
    qg_ref,
    kg_ref,
    tok_ref,
    fg_ref,
    route_t_ref,
    rw_ref,
    wgu,
    wd,
    wo,
    og,
    slots,
    hidden,
    part,
    rs1,
    half,
    rs2,
    home,
    back,
    kvs,
    qp,
    att,
    mpart,
    mrs1,
    mhalf,
    mrs2,
    passing,
    in_sem,
    w_sem,
    a2a_s,
    a2a_r,
    f1_s,
    f1_r,
    f2_s,
    f2_r,
    f3_s,
    f3_r,
    kva_s,
    kva_r,
    kvb_s,
    kvb_r,
    r1_s,
    r1_r,
    r2_s,
    r2_r,
    bk_s,
    bk_r,
    m1_s,
    m1_r,
    m2_s,
    m2_r,
    y2_s,
    y2_r,
):
    ep, tp, cap, groups, tile = dims
    f32, bf16 = jnp.float32, jnp.bfloat16
    per = ep // groups
    order = peer_order(ep)
    place = {mask: i for i, mask in enumerate(order)}
    e = lax.axis_index("ep")
    t = lax.axis_index("tp")
    t1 = t + 1 - 2 * (t % 2)
    t2 = (t + 2) % tp
    own_rows, width = tok_ref.shape
    head_size, rows = k_ref.shape
    heads = q_ref.shape[1] // head_size
    units = hidden.shape[1]
    lane_tile = wgu.shape[2] // 2
    half_ep = ep // 2

    def peer(mask):
        other, bit = e, 1
        while bit < ep:
            if mask & bit:
                other = other + bit * (1 - 2 * ((e // bit) % 2))
            bit *= 2
        return other

    def remote(src, dst, ssem, rsem, pe, pt):
        return pltpu.make_async_remote_copy(
            src_ref=src,
            dst_ref=dst,
            send_sem=ssem,
            recv_sem=rsem,
            device_id={"ep": pe, "tp": pt},
            device_id_type=pl.DeviceIdType.MESH,
        )

    def landed(ref, sem):
        pltpu.make_async_copy(ref, ref, sem).wait()

    barrier = pltpu.get_barrier_semaphore()
    peers = [(peer(mask), t) for mask in range(1, ep)] + [(e, t1), (e, t2)]
    for pe, pt in peers:
        pl.semaphore_signal(
            barrier, inc=1, device_id={"ep": pe, "tp": pt}, device_id_type=pl.DeviceIdType.MESH
        )

    routed = [
        pltpu.make_async_copy(source, target, in_sem.at[n])
        for n, (source, target) in enumerate(
            (
                (route_hbm, route_t_ref),
                (tok_hbm, tok_ref),
                (fg_hbm, fg_ref),
                (rw_hbm, rw_ref),
            )
        )
    ]
    attended = [
        pltpu.make_async_copy(source, target, in_sem.at[len(routed) + n])
        for n, (source, target) in enumerate(
            (
                (k_hbm, k_ref),
                (v_hbm, v_ref),
                (kg_hbm, kg_ref),
                (qg_hbm, qg_ref),
                (q_hbm, q_ref),
            )
        )
    ]
    for copy in routed + attended:
        copy.start()
    for copy in routed + attended:
        copy.wait()
    for n in range(units // lane_tile):
        cols = pl.ds(n * lane_tile, lane_tile)
        for side, source in ((0, gate_hbm), (lane_tile, up_hbm)):
            pltpu.make_async_copy(
                source.at[0, :, cols], wgu.at[n, :, pl.ds(side, lane_tile)], w_sem.at[0]
            ).start()
    load_down = pltpu.make_async_copy(down_hbm.at[0], wd, w_sem.at[1])
    load_out = pltpu.make_async_copy(ow_hbm, wo, w_sem.at[2])
    load_down.start()
    load_out.start()

    slot_rows = ep * cap
    later = lax.broadcasted_iota(jnp.int32, (own_rows, own_rows), 0)
    early = lax.broadcasted_iota(jnp.int32, (own_rows, own_rows), 1)
    picks = []
    sends = jnp.zeros((slot_rows, own_rows), f32)
    topk = route_t_ref.shape[0]
    diag = later == early

    def column(row):
        return jnp.sum(jnp.where(diag, row, jnp.zeros_like(row)), axis=1, keepdims=True)

    def position_of(expert):
        spot = jnp.zeros_like(expert)
        for mask in range(ep):
            spot += jnp.where(expert == peer(mask), place[mask], 0)
        return spot

    mix_weights = [column(rw_ref[k : k + 1, :]) for k in range(topk)]
    columns = [column(route_t_ref[k : k + 1, :]) for k in range(topk)]
    for k in range(topk):
        col = columns[k]
        row = route_t_ref[k : k + 1, :]
        rank_col = jnp.zeros((own_rows, 1), f32)
        rank_row = jnp.zeros((1, own_rows), f32)
        for other in range(topk):
            same = (col == route_t_ref[other : other + 1, :]) & (early < later)
            rank_col += jnp.sum(jnp.where(same, 1.0, 0.0), axis=1, keepdims=True)
            same_t = (columns[other] == row) & (later < early)
            rank_row += jnp.sum(jnp.where(same_t, 1.0, 0.0), axis=0, keepdims=True)
        slot_col = (position_of(col) * cap).astype(f32) + rank_col
        slot_row = (position_of(row) * cap).astype(f32) + rank_row
        lanes = lax.broadcasted_iota(jnp.int32, (own_rows, slot_rows), 1).astype(f32)
        picks.append(jnp.where(lanes == slot_col, 1.0, 0.0).astype(bf16))
        subs = lax.broadcasted_iota(jnp.int32, (slot_rows, own_rows), 0).astype(f32)
        sends += jnp.where(subs == slot_row, 1.0, 0.0)
    tok = tok_ref[...].astype(f32)
    normed = (
        tok * lax.rsqrt(jnp.mean(tok * tok, axis=-1, keepdims=True) + EPS) * fg_ref[...]
    ).astype(bf16)
    outgoing = (
        jnp.dot(sends.astype(bf16), normed, preferred_element_type=f32)
        .astype(bf16)
        .reshape(ep, cap, width)
    )
    og[...] = outgoing
    slots[place[0] // per, 0, place[0] % per] = outgoing[place[0]]

    with jax.named_scope("barrier"):
        pl.semaphore_wait(barrier, len(peers))

    a2a, f1, f2, f3, y2 = {}, {}, {}, {}, {}
    for i in range(ep):
        g, m = i // per, i % per
        if order[i]:
            a2a[i] = remote(
                og.at[i], slots.at[g, 0, m], a2a_s, a2a_r.at[i], peer(order[i]), t
            )
        f1[i] = remote(slots.at[g, 0, m], slots.at[g, 1, m], f1_s, f1_r.at[g], e, t1)
        mask = order[i]
        if 0 < mask < half_ep:
            f2[i] = remote(og.at[i], passing.at[mask], f2_s, f2_r.at[i], e, t2)
            y2[i] = remote(
                passing.at[mask], slots.at[g, 2, m], y2_s, y2_r.at[mask], peer(mask), t
            )
        else:
            f2[i] = remote(slots.at[g, 0, m], slots.at[g, 2, m], f2_s, f2_r.at[i], e, t2)
        f3[i] = remote(slots.at[g, 2, m], slots.at[g, 3, m], f3_s, f3_r.at[g], e, t1)
    kva, kvb = {}, {}
    for k in range(half_ep):
        kvb[k] = remote(kvs.at[0, k], kvs.at[1, k], kvb_s, kvb_r, peer(1), t)
        if k in (1, 2):
            kva[k] = remote(
                kvs.at[0, 0], kvs.at[0, k], kva_s, kva_r.at[k], peer(2 * k), t
            )
        if k == 3:
            kva[k] = remote(
                kvs.at[0, 2], kvs.at[0, 3], kva_s, kva_r.at[k], peer(2), t
            )

    near, far = issue_order(ep)
    for mask in near:
        a2a[place[mask]].start()
    for mask in range(1, half_ep):
        f2[place[mask]].start()
    for mask in far:
        a2a[place[mask]].start()

    def forward(mask):
        i = place[mask]
        with jax.named_scope(f"fwd{mask}"):
            if mask:
                a2a[i].wait_recv()
            if not 0 < mask < half_ep:
                f2[i].start()
            f1[i].start()

    def pass_on(mask):
        i = place[mask]
        with jax.named_scope(f"pass{mask}"):
            f2[i].wait_recv()
            y2[i].start()

    def relay(mask):
        i = place[mask]
        with jax.named_scope(f"relay{mask}"):
            (y2[i] if 0 < mask < half_ep else f2[i]).wait_recv()
            f3[i].start()

    forward(0)

    position = e * rows + lax.broadcasted_iota(jnp.int32, (rows, head_size), 0)
    channel = lax.broadcasted_iota(jnp.int32, (rows, head_size), 1)
    quarter = head_size // 4
    power = (channel // 2) % quarter
    freq = jnp.exp(power.astype(f32) * (-math.log(THETA) / quarter))
    grid_row = position // GRID_W
    spot = jnp.where(channel < head_size // 2, grid_row, position - grid_row * GRID_W)
    angle = spot.astype(f32) * freq
    cosine = jnp.cos(angle)
    sine = jnp.sin(angle) * jnp.where(channel % 2 == 0, -1.0, 1.0)
    both = jnp.concatenate([k_ref[...], v_ref[...]], axis=0).astype(f32).T
    rot_k = norm_rotate(both[:, :head_size], kg_ref[...], cosine, sine)
    kvs[0, 0, :, pl.ds(0, head_size)] = rot_k.astype(bf16)
    kvs[0, 0, :, pl.ds(head_size, head_size)] = both[:, head_size:].astype(bf16)

    kvb[0].start()

    for h in range(heads):
        lanes = pl.ds(h * head_size, head_size)
        turned = norm_rotate(q_ref[:, lanes].astype(f32), qg_ref[...], cosine, sine)
        qp[h, :, pl.ds(0, head_size)] = turned.astype(bf16)
        qp[h, :, pl.ds(head_size, head_size)] = jnp.zeros((rows, head_size), bf16)

    def share_keys(k):
        with jax.named_scope(f"share{k}"):
            kva[k].wait_recv()
            if k == 2:
                kva[3].start()
            kvb[k].start()

    scale = head_size ** (-0.5) * math.log2(math.e)
    half_rows = rows // 2
    y = t // 2
    stack = 2

    def attend(side, h):
        start = pl.multiple_of(side * half_rows, half_rows)
        joined = kvs[...].reshape(ep * rows, 2 * head_size)
        chosen = qp[pl.ds(h, stack), pl.ds(start, half_rows), :]
        scores = lax.dot_general(
            chosen.reshape(stack * half_rows, 2 * head_size),
            joined,
            (((1,), (1,)), ((), ())),
            preferred_element_type=f32,
        )
        expo = jnp.exp2((scores - jnp.max(scores, axis=-1, keepdims=True)) * scale)
        denom = jnp.sum(expo, axis=-1, keepdims=True)
        numer = jnp.dot(expo.astype(bf16), joined, preferred_element_type=f32)
        result = (numer[:, head_size:] / denom).astype(bf16)
        for k in range(stack):
            att[pl.ds(start, half_rows), pl.ds((h + k) * head_size, head_size)] = result[
                k * half_rows : (k + 1) * half_rows
            ]

    mrows = rows // tp
    homes = [t, t1, t2, (t1 + 2) % tp]
    m1 = [
        remote(mpart.at[2 * i + 1], mrs1.at[i], m1_s, m1_r.at[i], e, t1) for i in range(2)
    ]
    m2 = remote(mhalf, mrs2, m2_s, m2_r, e, t2)

    def project(js):
        for j in js:
            piece = att[pl.ds(pl.multiple_of(homes[j] * mrows, mrows), mrows), :]
            mpart[j] = jnp.dot(piece, wo[...], preferred_element_type=f32).astype(bf16)
            if j % 2:
                m1[j // 2].start()

    def feed_wait(g):
        with jax.named_scope(f"feedwait{g}"):
            landed(slots.at[g, 1], f1_r.at[g])
            landed(slots.at[g, 3], f3_r.at[g])

    rows_g = tp * per * cap

    def up(g):
        with jax.named_scope(f"up{g}"):
            chosen = slots[g].reshape(rows_g, width)
            for n in range(units // lane_tile):
                both = jnp.dot(chosen, wgu[n], preferred_element_type=f32)
                gate = both[:, :lane_tile]
                act = gate / (1.0 + jnp.exp(-gate)) * both[:, lane_tile:]
                hidden[:, pl.ds(n * lane_tile, lane_tile)] = act.astype(bf16)

    def down(g):
        with jax.named_scope(f"down{g}"):
            for n in range(width // tile):
                cols = pl.ds(n * tile, tile)
                result = jnp.dot(hidden[...], wd[:, cols], preferred_element_type=f32)
                part[g, :, :, :, cols] = result.astype(bf16).reshape(tp, per, cap, tile)
        r1[g, 1].start()
        r1[g, 0].start()

    r1, r2 = {}, {}
    for g in range(groups):
        for i in range(2):
            r1[g, i] = remote(
                part.at[g, 2 * i + 1], rs1.at[g, i], r1_s, r1_r.at[g, i], e, t1
            )
        r2[g] = remote(half.at[g], rs2.at[g], r2_s, r2_r.at[g], e, t2)
    bk = {}
    for i in range(ep):
        if order[i]:
            bk[i] = remote(
                home.at[i // per, i % per], back.at[i], bk_s, bk_r, peer(order[i]), t
            )

    def pair_sum(g):
        with jax.named_scope(f"pairsum{g}"):
            r1[g, 1].wait_recv()
            half[g] = (part[g, 2].astype(f32) + rs1[g, 1].astype(f32)).astype(bf16)
            r2[g].start()

    def finish(g):
        with jax.named_scope(f"finish{g}"):
            r1[g, 0].wait_recv()
            r2[g].wait_recv()
            total = (
                part[g, 0].astype(f32) + rs1[g, 0].astype(f32) + rs2[g].astype(f32)
            ).astype(bf16)
            home[g] = total
            for i in range(g * per, (g + 1) * per):
                if order[i]:
                    bk[i].start()
                else:
                    back[i] = total[i % per]

    def mixer_half():
        with jax.named_scope("mixhalf"):
            m1[1].wait_recv()
            mhalf[...] = (mpart[2].astype(f32) + mrs1[1].astype(f32)).astype(bf16)
            m2.start()

    kva[2].start()
    pass_on(1)
    forward(1)
    pass_on(2)
    pass_on(3)
    kva[1].start()
    relay(1)
    forward(4)
    forward(2)
    forward(3)
    relay(0)
    pltpu.make_async_copy(wgu, wgu, w_sem.at[0]).wait()
    load_down.wait()
    relay(4)
    forward(5)
    feed_wait(0)
    up(0)
    relay(2)
    forward(6)
    down(0)
    forward(7)
    relay(5)
    feed_wait(1)
    share_keys(2)
    up(1)
    pair_sum(0)
    relay(3)
    relay(6)
    down(1)
    relay(7)
    share_keys(1)
    feed_wait(2)
    up(2)
    share_keys(3)
    pair_sum(1)
    down(2)
    feed_wait(3)
    up(3)
    finish(0)
    pair_sum(2)
    down(3)
    with jax.named_scope("kvwait"):
        landed(kvs.at[1], kvb_r)
    with jax.named_scope("att0"):
        attend(1 - y, 0)
    pair_sum(3)
    finish(1)
    with jax.named_scope("att1"):
        attend(1 - y, 2)
    load_out.wait()
    with jax.named_scope("project"):
        project((3, 2))
    with jax.named_scope("att2"):
        attend(y, 0)
    mixer_half()
    finish(2)
    with jax.named_scope("att3"):
        attend(y, 2)
    with jax.named_scope("project"):
        project((1, 0))
    finish(3)
    others = pl.ds(0, ep - 1)
    landed(og.at[others], a2a_s)
    for sem in (f1_s, f2_s, f3_s):
        landed(og, sem)
    landed(og.at[pl.ds(0, half_ep - 1)], y2_s)
    landed(kvs.at[0, pl.ds(0, half_ep - 1)], kva_s)
    landed(kvs.at[0], kvb_s)
    landed(rs1, r1_s)
    landed(rs2, r2_s)
    with jax.named_scope("bkwait"):
        landed(back.at[pl.ds(0, ep - 1)], bk_r)
    returned = back[...].reshape(slot_rows, width)
    chosen = jnp.dot(jnp.concatenate(picks, axis=0), returned, preferred_element_type=f32)
    mixed = jnp.zeros((own_rows, width), f32)
    for k in range(topk):
        mixed += mix_weights[k] * chosen[k * own_rows : (k + 1) * own_rows]
    out_ref[...] = mixed.astype(bf16)
    with jax.named_scope("mwait"):
        m1[0].wait_recv()
        m2.wait_recv()
    mix_ref[...] = (
        mpart[0].astype(f32) + mrs1[0].astype(f32) + mrs2[...].astype(f32)
    ).astype(bf16)
    landed(og.at[others], bk_s)
    landed(mrs1, m1_s)
    m2.wait_send()


def peer_order(ep):
    half = ep // 2
    near = tuple(range(1, half)) + (0,)
    return tuple(m for i, k in enumerate(near) for m in (k, half + i))


def issue_order(ep):
    return (1, 2, 3), tuple(range(4, ep))


def store_kernel(mix_ref, rows_ref, mix_out, rows_out, sems):
    copies = [
        pltpu.make_async_copy(mix_ref, mix_out, sems.at[0]),
        pltpu.make_async_copy(rows_ref, rows_out, sems.at[1]),
    ]
    for copy in copies:
        copy.start()
    for copy in copies:
        copy.wait()


def local_fused(
    queries,
    keys,
    values,
    q_gain,
    k_gain,
    out_weight,
    tokens,
    ffn_gain,
    route,
    route_weight,
    gate_weight,
    up_weight,
    down_weight,
):
    ep = lax.axis_size("ep")
    tp = lax.axis_size("tp")
    rows = queries.shape[0]
    head_size = q_gain.shape[0]
    heads = queries.shape[1] // head_size
    own_rows, width = tokens.shape
    cap = 2 * own_rows * route.shape[1] // ep
    units = gate_weight.shape[2]
    lane_tile = 128
    tile = math.gcd(width, 512)
    groups = GROUPS
    per = ep // groups
    bf16 = jnp.bfloat16
    vmem = pl.BlockSpec(memory_space=pltpu.VMEM)
    hbm = pl.BlockSpec(memory_space=pl.ANY)
    dma = pltpu.SemaphoreType.DMA
    mrows = rows // tp
    flops = 2 * tp * ep * cap * width * units * 3 + 4 * heads * rows * rows * ep * head_size
    loaded = (
        queries,
        keys.T,
        values.T,
        q_gain[None, :],
        k_gain[None, :],
        tokens,
        ffn_gain[None, :],
        route.T,
        route_weight.T,
    )
    held = pl.pallas_call(
        functools.partial(fused_kernel, (ep, tp, cap, groups, tile)),
        out_shape=(
            pltpu.VMEM((mrows, width), bf16),
            pltpu.VMEM((own_rows, width), bf16),
        ),
        in_specs=[hbm] * 13,
        out_specs=(vmem, vmem),
        scratch_shapes=[pltpu.VMEM(part.shape, part.dtype) for part in loaded]
        + [
            pltpu.VMEM((units // lane_tile, width, 2 * lane_tile), bf16),
            pltpu.VMEM((units, width), bf16),
            pltpu.VMEM(out_weight.shape, bf16),
            pltpu.VMEM((ep, cap, width), bf16),
            pltpu.VMEM((groups, tp, per, cap, width), bf16),
            pltpu.VMEM((tp * per * cap, units), bf16),
            pltpu.VMEM((groups, tp, per, cap, width), bf16),
            pltpu.VMEM((groups, 2, per, cap, width), bf16),
            pltpu.VMEM((groups, per, cap, width), bf16),
            pltpu.VMEM((groups, per, cap, width), bf16),
            pltpu.VMEM((groups, per, cap, width), bf16),
            pltpu.VMEM((ep, cap, width), bf16),
            pltpu.VMEM((2, ep // 2, rows, 2 * head_size), bf16),
            pltpu.VMEM((heads, rows, 2 * head_size), bf16),
            pltpu.VMEM((rows, heads * head_size), bf16),
            pltpu.VMEM((tp, mrows, width), bf16),
            pltpu.VMEM((2, mrows, width), bf16),
            pltpu.VMEM((mrows, width), bf16),
            pltpu.VMEM((mrows, width), bf16),
            pltpu.VMEM((ep // 2, cap, width), bf16),
            dma((len(loaded),)),
            dma((3,)),
        ]
        + [dma, dma((ep,)), dma, dma((groups,)), dma, dma((ep,)), dma, dma((groups,))]
        + [dma, dma((ep // 2,)), dma, dma]
        + [dma, dma((groups, 2)), dma, dma((groups,)), dma, dma]
        + [dma, dma((2,)), dma, dma]
        + [dma, dma((ep // 2,))],
        compiler_params=pltpu.CompilerParams(
            collective_id=0, has_side_effects=True, vmem_limit_bytes=60 * 1024 * 1024
        ),
        cost_estimate=pl.CostEstimate(
            flops=flops, bytes_accessed=3 * 2 * width * units, transcendentals=0
        ),
    )(
        *loaded,
        gate_weight,
        up_weight,
        down_weight,
        out_weight,
    )
    return pl.pallas_call(
        store_kernel,
        out_shape=tuple(jax.ShapeDtypeStruct(part.shape, bf16) for part in held),
        in_specs=[vmem] * len(held),
        out_specs=(hbm,) * len(held),
        scratch_shapes=[dma((len(held),))],
    )(*[pltpu.with_memory_space_constraint(part, pltpu.VMEM) for part in held])


GROUPS = 4


def step(*args):
    queries, keys, q_gain, tokens, route, gate_weight = (args[i] for i in (0, 1, 3, 6, 8, 10))
    ep, tp = lax.axis_size("ep"), lax.axis_size("tp")
    cap = 2 * tokens.shape[0] * route.shape[1] // ep
    fits = (
        tp == 4
        and ep == 8
        and queries.shape[1] % (2 * q_gain.shape[0]) == 0
        and ep % GROUPS == 0
        and cap % 16 == 0
        and keys.shape[1] == q_gain.shape[0]
        and gate_weight.shape[2] % 128 == 0
        and queries.shape[0] % (16 * tp) == 0
    )
    return local_fused(*args) if fits else local(*args)


def solution(mesh):
    placed = (
        P("ep", "tp"),
        P("ep", "tp"),
        P("ep", "tp"),
        P(),
        P(),
        P("tp", None),
        P(("ep", "tp"), None),
        P(),
        P(("ep", "tp"), None),
        P(("ep", "tp"), None),
        P("ep", None, "tp"),
        P("ep", None, "tp"),
        P("ep", "tp", None),
    )
    return jax.shard_map(
        step,
        mesh=mesh,
        in_specs=placed,
        out_specs=(P(("ep", "tp"), None), P(("ep", "tp"), None)),
        check_vma=False,
    )
```

```python
import functools
import math

import jax
import jax.numpy as jnp
from jax import lax
from jax.experimental import pallas as pl
from jax.experimental.pallas import tpu as pltpu
from jax.sharding import PartitionSpec as P

GRID_W = 64


EPS = 1e-06
THETA = 10000.0


def head_norm(vals, gain):
    vals = vals.astype(jnp.float32)
    return vals * lax.rsqrt(jnp.mean(vals * vals, axis=-1, keepdims=True) + EPS) * gain


def rotate(vals, positions):
    pairs = vals.shape[-1] // 2
    quarter = pairs // 2
    freqs = THETA ** (-jnp.arange(quarter, dtype=jnp.float32) / quarter)
    grid_row = (positions // GRID_W).astype(jnp.float32)
    grid_col = (positions % GRID_W).astype(jnp.float32)
    angle = jnp.concatenate([grid_row[:, None] * freqs, grid_col[:, None] * freqs], axis=-1)
    cosine = jnp.cos(angle)[:, None, :]
    sine = jnp.sin(angle)[:, None, :]
    split = vals.reshape(vals.shape[:-1] + (pairs, 2))
    first = split[..., 0]
    second = split[..., 1]
    turned = jnp.stack([first * cosine - second * sine, first * sine + second * cosine], axis=-1)
    return turned.reshape(vals.shape)


def local(
    queries,
    keys,
    values,
    q_gain,
    k_gain,
    out_weight,
    tokens,
    ffn_gain,
    route,
    route_weight,
    gate_weight,
    up_weight,
    down_weight,
):
    local_rows = queries.shape[0]
    head_size = q_gain.shape[0]
    query_heads = queries.shape[1] // head_size
    key_heads = keys.shape[1] // head_size
    group = query_heads // key_heads
    key_width = key_heads * head_size
    positions = lax.axis_index("ep") * local_rows + jnp.arange(local_rows, dtype=jnp.int32)
    rot_q = rotate(
        head_norm(queries.reshape(local_rows, query_heads, head_size), q_gain), positions
    ).astype(jnp.bfloat16)
    rot_q = rot_q.reshape(local_rows, key_heads, group, head_size)
    rot_k = rotate(
        head_norm(keys.reshape(local_rows, key_heads, head_size), k_gain), positions
    ).astype(jnp.bfloat16)
    joined = jnp.concatenate([rot_k.reshape(local_rows, key_width), values], axis=1)
    scale = head_size ** (-0.5)

    def fold_block(carry, block):
        highest, denom, numer = carry
        key_block = block[:, :key_width].reshape(-1, key_heads, head_size)
        value_block = block[:, key_width:].reshape(-1, key_heads, head_size)
        scores = (
            jnp.einsum("qkgd,skd->qkgs", rot_q, key_block, preferred_element_type=jnp.float32)
            * scale
        )
        new_high = jnp.maximum(highest, jnp.max(scores, axis=-1))
        shrink = jnp.exp(highest - new_high)
        expo = jnp.exp(scores - new_high[..., None])
        denom = denom * shrink + jnp.sum(expo, axis=-1)
        numer = numer * shrink[..., None] + jnp.einsum(
            "qkgs,skd->qkgd",
            expo.astype(jnp.bfloat16),
            value_block,
            preferred_element_type=jnp.float32,
        )
        return ((new_high, denom, numer), None)

    start_high = jnp.full((local_rows, key_heads, group), -1e30, jnp.float32)
    start_denom = jnp.zeros((local_rows, key_heads, group), jnp.float32)
    start_numer = jnp.zeros((local_rows, key_heads, group, head_size), jnp.float32)
    carry = (start_high, start_denom, start_numer)
    piece = lax.all_gather(joined, "ep", axis=0, tiled=True)
    length = piece.shape[0]
    size = length
    while size > 2048 and size % 2 == 0:
        size = size // 2
    blocks = piece.reshape(length // size, size, piece.shape[1])
    carry, _ = lax.scan(fold_block, carry, blocks)
    highest, denom, numer = carry
    attended = (
        (numer / denom[..., None]).astype(jnp.bfloat16).reshape(local_rows, query_heads * head_size)
    )
    own_rows = tokens.shape[0]
    width = tokens.shape[1]
    picks_row = route.shape[1]
    experts = lax.axis_size("ep")
    capacity = 2 * own_rows * picks_row // experts
    token_float = tokens.astype(jnp.float32)
    normed = (
        token_float
        * lax.rsqrt(jnp.mean(token_float * token_float, axis=-1, keepdims=True) + EPS)
        * ffn_gain
    ).astype(jnp.bfloat16)
    flat_route = route.reshape(-1)
    expert_hot = (flat_route[:, None] == jnp.arange(experts, dtype=jnp.int32)[None, :]).astype(
        jnp.int32
    )
    earlier = jnp.cumsum(expert_hot, axis=0) - expert_hot
    rank = jnp.sum(earlier * expert_hot, axis=1)
    slot = flat_route * capacity + rank
    pick_hot = (slot[:, None] == jnp.arange(experts * capacity, dtype=jnp.int32)[None, :]).astype(
        jnp.bfloat16
    )
    row_hot = jnp.sum(pick_hot.reshape(own_rows, picks_row, experts * capacity), axis=1)
    outgoing = jnp.einsum("rs,rd->sd", row_hot, normed, preferred_element_type=jnp.float32).astype(
        jnp.bfloat16
    )
    outgoing = outgoing.reshape(experts, capacity, width)
    gate_local = gate_weight[0]
    up_local = up_weight[0]
    down_local = down_weight[0]
    arrived = lax.all_to_all(outgoing, "ep", split_axis=0, concat_axis=0, tiled=True)
    sources = arrived.shape[0]
    items = arrived.shape[1]
    slot_rows = arrived.reshape(sources * items, width)
    piece = lax.all_gather(slot_rows, "tp", axis=0, tiled=True)
    gate = jnp.dot(piece, gate_local, preferred_element_type=jnp.float32)
    upper = jnp.dot(piece, up_local, preferred_element_type=jnp.float32)
    hidden = (jax.nn.silu(gate) * upper).astype(jnp.bfloat16)
    worked = jnp.dot(hidden, down_local, preferred_element_type=jnp.float32).reshape(
        -1, items, width
    )
    head_partial = jnp.dot(attended, out_weight, preferred_element_type=jnp.float32)
    mixer_sum, expert_sum = (
        lax.psum_scatter(
            head_partial.astype(jnp.bfloat16), "tp", scatter_dimension=0, tiled=True
        ).astype(jnp.float32),
        lax.psum_scatter(worked.astype(jnp.bfloat16), "tp", scatter_dimension=0, tiled=True).astype(
            jnp.float32
        ),
    )
    mixer_out = mixer_sum.astype(jnp.bfloat16)
    home = expert_sum.astype(jnp.bfloat16)
    back = lax.all_to_all(home, "ep", split_axis=0, concat_axis=0, tiled=True)
    copies = jnp.dot(
        pick_hot, back.reshape(experts * capacity, width), preferred_element_type=jnp.float32
    )
    weighted = route_weight[..., None] * copies.reshape(own_rows, picks_row, width)
    mixed = jnp.sum(weighted, axis=1).astype(jnp.bfloat16)
    return (mixer_out, mixed)


def norm_rotate(vals, gain, cosine, sine):
    vals = vals * lax.rsqrt(jnp.mean(vals * vals, axis=-1, keepdims=True) + EPS) * gain
    size = vals.shape[-1]
    lane = lax.broadcasted_iota(jnp.int32, vals.shape, 1)
    up = jnp.concatenate([vals[:, 1:], vals[:, :1]], axis=1)
    down = jnp.concatenate([vals[:, size - 1 :], vals[:, : size - 1]], axis=1)
    swapped = jnp.where(lane % 2 == 0, up, down)
    return vals * cosine + swapped * sine


def fused_kernel(
    dims,
    q_hbm,
    k_hbm,
    v_hbm,
    qg_hbm,
    kg_hbm,
    tok_hbm,
    fg_hbm,
    route_hbm,
    rw_hbm,
    gate_hbm,
    up_hbm,
    down_hbm,
    ow_hbm,
    mix_ref,
    out_ref,
    q_ref,
    k_ref,
    v_ref,
    qg_ref,
    kg_ref,
    tok_ref,
    fg_ref,
    route_t_ref,
    rw_ref,
    wgu,
    wd,
    wo,
    og,
    slots,
    hidden,
    part,
    rs1,
    half,
    rs2,
    home,
    back,
    kvs,
    qp,
    att,
    mpart,
    mrs1,
    mhalf,
    mrs2,
    passing,
    in_sem,
    w_sem,
    a2a_s,
    a2a_r,
    f1_s,
    f1_r,
    f2_s,
    f2_r,
    f3_s,
    f3_r,
    kva_s,
    kva_r,
    kvb_s,
    kvb_r,
    r1_s,
    r1_r,
    r2_s,
    r2_r,
    bk_s,
    bk_r,
    m1_s,
    m1_r,
    m2_s,
    m2_r,
    y2_s,
    y2_r,
):
    ep, tp, cap, groups, tile = dims
    f32, bf16 = jnp.float32, jnp.bfloat16
    per = ep // groups
    order = peer_order(ep)
    place = {mask: i for i, mask in enumerate(order)}
    e = lax.axis_index("ep")
    t = lax.axis_index("tp")
    t1 = t + 1 - 2 * (t % 2)
    t2 = (t + 2) % tp
    own_rows, width = tok_ref.shape
    head_size, rows = k_ref.shape
    heads = q_ref.shape[1] // head_size
    units = hidden.shape[1]
    lane_tile = wgu.shape[2] // 2
    half_ep = ep // 2

    def peer(mask):
        other, bit = e, 1
        while bit < ep:
            if mask & bit:
                other = other + bit * (1 - 2 * ((e // bit) % 2))
            bit *= 2
        return other

    def remote(src, dst, ssem, rsem, pe, pt):
        return pltpu.make_async_remote_copy(
            src_ref=src,
            dst_ref=dst,
            send_sem=ssem,
            recv_sem=rsem,
            device_id={"ep": pe, "tp": pt},
            device_id_type=pl.DeviceIdType.MESH,
        )

    def landed(ref, sem):
        pltpu.make_async_copy(ref, ref, sem).wait()

    barrier = pltpu.get_barrier_semaphore()
    peers = [(peer(mask), t) for mask in range(1, ep)] + [(e, t1), (e, t2)]
    for pe, pt in peers:
        pl.semaphore_signal(
            barrier, inc=1, device_id={"ep": pe, "tp": pt}, device_id_type=pl.DeviceIdType.MESH
        )

    routed = [
        pltpu.make_async_copy(source, target, in_sem.at[n])
        for n, (source, target) in enumerate(
            (
                (route_hbm, route_t_ref),
                (tok_hbm, tok_ref),
                (fg_hbm, fg_ref),
                (rw_hbm, rw_ref),
            )
        )
    ]
    attended = [
        pltpu.make_async_copy(source, target, in_sem.at[len(routed) + n])
        for n, (source, target) in enumerate(
            (
                (k_hbm, k_ref),
                (v_hbm, v_ref),
                (kg_hbm, kg_ref),
                (qg_hbm, qg_ref),
                (q_hbm, q_ref),
            )
        )
    ]
    for copy in routed + attended:
        copy.start()
    for copy in routed + attended:
        copy.wait()
    for n in range(units // lane_tile):
        cols = pl.ds(n * lane_tile, lane_tile)
        for side, source in ((0, gate_hbm), (lane_tile, up_hbm)):
            pltpu.make_async_copy(
                source.at[0, :, cols], wgu.at[n, :, pl.ds(side, lane_tile)], w_sem.at[0]
            ).start()
    load_down = pltpu.make_async_copy(down_hbm.at[0], wd, w_sem.at[1])
    load_out = pltpu.make_async_copy(ow_hbm, wo, w_sem.at[2])
    load_down.start()
    load_out.start()

    slot_rows = ep * cap
    later = lax.broadcasted_iota(jnp.int32, (own_rows, own_rows), 0)
    early = lax.broadcasted_iota(jnp.int32, (own_rows, own_rows), 1)
    picks = []
    sends = jnp.zeros((slot_rows, own_rows), f32)
    topk = route_t_ref.shape[0]
    diag = later == early

    def column(row):
        return jnp.sum(jnp.where(diag, row, jnp.zeros_like(row)), axis=1, keepdims=True)

    def position_of(expert):
        spot = jnp.zeros_like(expert)
        for mask in range(ep):
            spot += jnp.where(expert == peer(mask), place[mask], 0)
        return spot

    mix_weights = [column(rw_ref[k : k + 1, :]) for k in range(topk)]
    columns = [column(route_t_ref[k : k + 1, :]) for k in range(topk)]
    for k in range(topk):
        col = columns[k]
        row = route_t_ref[k : k + 1, :]
        rank_col = jnp.zeros((own_rows, 1), f32)
        rank_row = jnp.zeros((1, own_rows), f32)
        for other in range(topk):
            same = (col == route_t_ref[other : other + 1, :]) & (early < later)
            rank_col += jnp.sum(jnp.where(same, 1.0, 0.0), axis=1, keepdims=True)
            same_t = (columns[other] == row) & (later < early)
            rank_row += jnp.sum(jnp.where(same_t, 1.0, 0.0), axis=0, keepdims=True)
        slot_col = (position_of(col) * cap).astype(f32) + rank_col
        slot_row = (position_of(row) * cap).astype(f32) + rank_row
        lanes = lax.broadcasted_iota(jnp.int32, (own_rows, slot_rows), 1).astype(f32)
        picks.append(jnp.where(lanes == slot_col, 1.0, 0.0).astype(bf16))
        subs = lax.broadcasted_iota(jnp.int32, (slot_rows, own_rows), 0).astype(f32)
        sends += jnp.where(subs == slot_row, 1.0, 0.0)
    tok = tok_ref[...].astype(f32)
    normed = (
        tok * lax.rsqrt(jnp.mean(tok * tok, axis=-1, keepdims=True) + EPS) * fg_ref[...]
    ).astype(bf16)
    outgoing = (
        jnp.dot(sends.astype(bf16), normed, preferred_element_type=f32)
        .astype(bf16)
        .reshape(ep, cap, width)
    )
    og[...] = outgoing
    slots[place[0] // per, 0, place[0] % per] = outgoing[place[0]]

    with jax.named_scope("barrier"):
        pl.semaphore_wait(barrier, len(peers))

    a2a, f1, f2, f3, y2 = {}, {}, {}, {}, {}
    for i in range(ep):
        g, m = i // per, i % per
        if order[i]:
            a2a[i] = remote(
                og.at[i], slots.at[g, 0, m], a2a_s, a2a_r.at[i], peer(order[i]), t
            )
        f1[i] = remote(slots.at[g, 0, m], slots.at[g, 1, m], f1_s, f1_r.at[g], e, t1)
        mask = order[i]
        if 0 < mask < half_ep:
            f2[i] = remote(og.at[i], passing.at[mask], f2_s, f2_r.at[i], e, t2)
            y2[i] = remote(
                passing.at[mask], slots.at[g, 2, m], y2_s, y2_r.at[mask], peer(mask), t
            )
        else:
            f2[i] = remote(slots.at[g, 0, m], slots.at[g, 2, m], f2_s, f2_r.at[i], e, t2)
        f3[i] = remote(slots.at[g, 2, m], slots.at[g, 3, m], f3_s, f3_r.at[g], e, t1)
    kva, kvb = {}, {}
    for k in range(half_ep):
        kvb[k] = remote(kvs.at[0, k], kvs.at[1, k], kvb_s, kvb_r, peer(1), t)
        if k in (1, 2):
            kva[k] = remote(
                kvs.at[0, 0], kvs.at[0, k], kva_s, kva_r.at[k], peer(2 * k), t
            )
        if k == 3:
            kva[k] = remote(
                kvs.at[0, 2], kvs.at[0, 3], kva_s, kva_r.at[k], peer(2), t
            )

    near, far = issue_order(ep)
    for mask in near:
        a2a[place[mask]].start()
    for mask in range(1, half_ep):
        f2[place[mask]].start()
    for mask in far:
        a2a[place[mask]].start()

    def forward(mask):
        i = place[mask]
        with jax.named_scope(f"fwd{mask}"):
            if mask:
                a2a[i].wait_recv()
            if not 0 < mask < half_ep:
                f2[i].start()
            f1[i].start()

    def pass_on(mask):
        i = place[mask]
        with jax.named_scope(f"pass{mask}"):
            f2[i].wait_recv()
            y2[i].start()

    def relay(mask):
        i = place[mask]
        with jax.named_scope(f"relay{mask}"):
            (y2[i] if 0 < mask < half_ep else f2[i]).wait_recv()
            f3[i].start()

    forward(0)

    position = e * rows + lax.broadcasted_iota(jnp.int32, (rows, head_size), 0)
    channel = lax.broadcasted_iota(jnp.int32, (rows, head_size), 1)
    quarter = head_size // 4
    power = (channel // 2) % quarter
    freq = jnp.exp(power.astype(f32) * (-math.log(THETA) / quarter))
    grid_row = position // GRID_W
    spot = jnp.where(channel < head_size // 2, grid_row, position - grid_row * GRID_W)
    angle = spot.astype(f32) * freq
    cosine = jnp.cos(angle)
    sine = jnp.sin(angle) * jnp.where(channel % 2 == 0, -1.0, 1.0)
    both = jnp.concatenate([k_ref[...], v_ref[...]], axis=0).astype(f32).T
    rot_k = norm_rotate(both[:, :head_size], kg_ref[...], cosine, sine)
    kvs[0, 0, :, pl.ds(0, head_size)] = rot_k.astype(bf16)
    kvs[0, 0, :, pl.ds(head_size, head_size)] = both[:, head_size:].astype(bf16)

    kvb[0].start()

    for h in range(heads):
        lanes = pl.ds(h * head_size, head_size)
        turned = norm_rotate(q_ref[:, lanes].astype(f32), qg_ref[...], cosine, sine)
        qp[h, :, pl.ds(0, head_size)] = turned.astype(bf16)
        qp[h, :, pl.ds(head_size, head_size)] = jnp.zeros((rows, head_size), bf16)

    def share_keys(k):
        with jax.named_scope(f"share{k}"):
            kva[k].wait_recv()
            if k == 2:
                kva[3].start()
            kvb[k].start()

    scale = head_size ** (-0.5) * math.log2(math.e)
    half_rows = rows // 2
    y = t // 2
    stack = 2

    def attend(side, h):
        start = pl.multiple_of(side * half_rows, half_rows)
        joined = kvs[...].reshape(ep * rows, 2 * head_size)
        chosen = qp[pl.ds(h, stack), pl.ds(start, half_rows), :]
        scores = lax.dot_general(
            chosen.reshape(stack * half_rows, 2 * head_size),
            joined,
            (((1,), (1,)), ((), ())),
            preferred_element_type=f32,
        )
        expo = jnp.exp2((scores - jnp.max(scores, axis=-1, keepdims=True)) * scale)
        denom = jnp.sum(expo, axis=-1, keepdims=True)
        numer = jnp.dot(expo.astype(bf16), joined, preferred_element_type=f32)
        result = (numer[:, head_size:] / denom).astype(bf16)
        for k in range(stack):
            att[pl.ds(start, half_rows), pl.ds((h + k) * head_size, head_size)] = result[
                k * half_rows : (k + 1) * half_rows
            ]

    mrows = rows // tp
    homes = [t, t1, t2, (t1 + 2) % tp]
    m1 = [
        remote(mpart.at[2 * i + 1], mrs1.at[i], m1_s, m1_r.at[i], e, t1) for i in range(2)
    ]
    m2 = remote(mhalf, mrs2, m2_s, m2_r, e, t2)

    def project(js):
        for j in js:
            piece = att[pl.ds(pl.multiple_of(homes[j] * mrows, mrows), mrows), :]
            mpart[j] = jnp.dot(piece, wo[...], preferred_element_type=f32).astype(bf16)
            if j % 2:
                m1[j // 2].start()

    def feed_wait(g):
        with jax.named_scope(f"feedwait{g}"):
            landed(slots.at[g, 1], f1_r.at[g])
            landed(slots.at[g, 3], f3_r.at[g])

    rows_g = tp * per * cap

    def up(g):
        with jax.named_scope(f"up{g}"):
            chosen = slots[g].reshape(rows_g, width)
            for n in range(units // lane_tile):
                both = jnp.dot(chosen, wgu[n], preferred_element_type=f32)
                gate = both[:, :lane_tile]
                act = gate / (1.0 + jnp.exp(-gate)) * both[:, lane_tile:]
                hidden[:, pl.ds(n * lane_tile, lane_tile)] = act.astype(bf16)

    def down(g):
        with jax.named_scope(f"down{g}"):
            for n in range(width // tile):
                cols = pl.ds(n * tile, tile)
                result = jnp.dot(hidden[...], wd[:, cols], preferred_element_type=f32)
                part[g, :, :, :, cols] = result.astype(bf16).reshape(tp, per, cap, tile)
        r1[g, 1].start()
        r1[g, 0].start()

    r1, r2 = {}, {}
    for g in range(groups):
        for i in range(2):
            r1[g, i] = remote(
                part.at[g, 2 * i + 1], rs1.at[g, i], r1_s, r1_r.at[g, i], e, t1
            )
        r2[g] = remote(half.at[g], rs2.at[g], r2_s, r2_r.at[g], e, t2)
    bk = {}
    for i in range(ep):
        if order[i]:
            bk[i] = remote(
                home.at[i // per, i % per], back.at[i], bk_s, bk_r, peer(order[i]), t
            )

    def pair_sum(g):
        with jax.named_scope(f"pairsum{g}"):
            r1[g, 1].wait_recv()
            half[g] = (part[g, 2].astype(f32) + rs1[g, 1].astype(f32)).astype(bf16)
            r2[g].start()

    def finish(g):
        with jax.named_scope(f"finish{g}"):
            r1[g, 0].wait_recv()
            r2[g].wait_recv()
            total = (
                part[g, 0].astype(f32) + rs1[g, 0].astype(f32) + rs2[g].astype(f32)
            ).astype(bf16)
            home[g] = total
            for i in range(g * per, (g + 1) * per):
                if order[i]:
                    bk[i].start()
                else:
                    back[i] = total[i % per]

    def mixer_half():
        with jax.named_scope("mixhalf"):
            m1[1].wait_recv()
            mhalf[...] = (mpart[2].astype(f32) + mrs1[1].astype(f32)).astype(bf16)
            m2.start()

    kva[2].start()
    pass_on(1)
    forward(1)
    pass_on(2)
    pass_on(3)
    kva[1].start()
    relay(1)
    forward(4)
    forward(2)
    forward(3)
    relay(0)
    pltpu.make_async_copy(wgu, wgu, w_sem.at[0]).wait()
    load_down.wait()
    relay(4)
    forward(5)
    feed_wait(0)
    up(0)
    relay(2)
    forward(6)
    down(0)
    forward(7)
    relay(5)
    feed_wait(1)
    pair_sum(0)
    share_keys(2)
    up(1)
    relay(3)
    relay(6)
    down(1)
    relay(7)
    share_keys(1)
    feed_wait(2)
    up(2)
    share_keys(3)
    pair_sum(1)
    down(2)
    feed_wait(3)
    up(3)
    finish(0)
    pair_sum(2)
    down(3)
    with jax.named_scope("kvwait"):
        landed(kvs.at[1], kvb_r)
    with jax.named_scope("att0"):
        attend(1 - y, 0)
    pair_sum(3)
    finish(1)
    with jax.named_scope("att1"):
        attend(1 - y, 2)
    load_out.wait()
    with jax.named_scope("project"):
        project((3, 2))
    with jax.named_scope("att2"):
        attend(y, 0)
    mixer_half()
    finish(2)
    with jax.named_scope("att3"):
        attend(y, 2)
    with jax.named_scope("project"):
        project((1, 0))
    finish(3)
    others = pl.ds(0, ep - 1)
    landed(og.at[others], a2a_s)
    for sem in (f1_s, f2_s, f3_s):
        landed(og, sem)
    landed(og.at[pl.ds(0, half_ep - 1)], y2_s)
    landed(kvs.at[0, pl.ds(0, half_ep - 1)], kva_s)
    landed(kvs.at[0], kvb_s)
    landed(rs1, r1_s)
    landed(rs2, r2_s)
    with jax.named_scope("bkwait"):
        landed(back.at[pl.ds(0, ep - 1)], bk_r)
    returned = back[...].reshape(slot_rows, width)
    chosen = jnp.dot(jnp.concatenate(picks, axis=0), returned, preferred_element_type=f32)
    mixed = jnp.zeros((own_rows, width), f32)
    for k in range(topk):
        mixed += mix_weights[k] * chosen[k * own_rows : (k + 1) * own_rows]
    out_ref[...] = mixed.astype(bf16)
    with jax.named_scope("mwait"):
        m1[0].wait_recv()
        m2.wait_recv()
    mix_ref[...] = (
        mpart[0].astype(f32) + mrs1[0].astype(f32) + mrs2[...].astype(f32)
    ).astype(bf16)
    landed(og.at[others], bk_s)
    landed(mrs1, m1_s)
    m2.wait_send()


def peer_order(ep):
    half = ep // 2
    near = tuple(range(1, half)) + (0,)
    return tuple(m for i, k in enumerate(near) for m in (k, half + i))


def issue_order(ep):
    return (1, 2, 3), tuple(range(4, ep))


def store_kernel(mix_ref, rows_ref, mix_out, rows_out, sems):
    copies = [
        pltpu.make_async_copy(mix_ref, mix_out, sems.at[0]),
        pltpu.make_async_copy(rows_ref, rows_out, sems.at[1]),
    ]
    for copy in copies:
        copy.start()
    for copy in copies:
        copy.wait()


def local_fused(
    queries,
    keys,
    values,
    q_gain,
    k_gain,
    out_weight,
    tokens,
    ffn_gain,
    route,
    route_weight,
    gate_weight,
    up_weight,
    down_weight,
):
    ep = lax.axis_size("ep")
    tp = lax.axis_size("tp")
    rows = queries.shape[0]
    head_size = q_gain.shape[0]
    heads = queries.shape[1] // head_size
    own_rows, width = tokens.shape
    cap = 2 * own_rows * route.shape[1] // ep
    units = gate_weight.shape[2]
    lane_tile = 128
    tile = math.gcd(width, 512)
    groups = GROUPS
    per = ep // groups
    bf16 = jnp.bfloat16
    vmem = pl.BlockSpec(memory_space=pltpu.VMEM)
    hbm = pl.BlockSpec(memory_space=pl.ANY)
    dma = pltpu.SemaphoreType.DMA
    mrows = rows // tp
    flops = 2 * tp * ep * cap * width * units * 3 + 4 * heads * rows * rows * ep * head_size
    loaded = (
        queries,
        keys.T,
        values.T,
        q_gain[None, :],
        k_gain[None, :],
        tokens,
        ffn_gain[None, :],
        route.T,
        route_weight.T,
    )
    held = pl.pallas_call(
        functools.partial(fused_kernel, (ep, tp, cap, groups, tile)),
        out_shape=(
            pltpu.VMEM((mrows, width), bf16),
            pltpu.VMEM((own_rows, width), bf16),
        ),
        in_specs=[hbm] * 13,
        out_specs=(vmem, vmem),
        scratch_shapes=[pltpu.VMEM(part.shape, part.dtype) for part in loaded]
        + [
            pltpu.VMEM((units // lane_tile, width, 2 * lane_tile), bf16),
            pltpu.VMEM((units, width), bf16),
            pltpu.VMEM(out_weight.shape, bf16),
            pltpu.VMEM((ep, cap, width), bf16),
            pltpu.VMEM((groups, tp, per, cap, width), bf16),
            pltpu.VMEM((tp * per * cap, units), bf16),
            pltpu.VMEM((groups, tp, per, cap, width), bf16),
            pltpu.VMEM((groups, 2, per, cap, width), bf16),
            pltpu.VMEM((groups, per, cap, width), bf16),
            pltpu.VMEM((groups, per, cap, width), bf16),
            pltpu.VMEM((groups, per, cap, width), bf16),
            pltpu.VMEM((ep, cap, width), bf16),
            pltpu.VMEM((2, ep // 2, rows, 2 * head_size), bf16),
            pltpu.VMEM((heads, rows, 2 * head_size), bf16),
            pltpu.VMEM((rows, heads * head_size), bf16),
            pltpu.VMEM((tp, mrows, width), bf16),
            pltpu.VMEM((2, mrows, width), bf16),
            pltpu.VMEM((mrows, width), bf16),
            pltpu.VMEM((mrows, width), bf16),
            pltpu.VMEM((ep // 2, cap, width), bf16),
            dma((len(loaded),)),
            dma((3,)),
        ]
        + [dma, dma((ep,)), dma, dma((groups,)), dma, dma((ep,)), dma, dma((groups,))]
        + [dma, dma((ep // 2,)), dma, dma]
        + [dma, dma((groups, 2)), dma, dma((groups,)), dma, dma]
        + [dma, dma((2,)), dma, dma]
        + [dma, dma((ep // 2,))],
        compiler_params=pltpu.CompilerParams(
            collective_id=0, has_side_effects=True, vmem_limit_bytes=60 * 1024 * 1024
        ),
        cost_estimate=pl.CostEstimate(
            flops=flops, bytes_accessed=3 * 2 * width * units, transcendentals=0
        ),
    )(
        *loaded,
        gate_weight,
        up_weight,
        down_weight,
        out_weight,
    )
    return pl.pallas_call(
        store_kernel,
        out_shape=tuple(jax.ShapeDtypeStruct(part.shape, bf16) for part in held),
        in_specs=[vmem] * len(held),
        out_specs=(hbm,) * len(held),
        scratch_shapes=[dma((len(held),))],
    )(*[pltpu.with_memory_space_constraint(part, pltpu.VMEM) for part in held])


GROUPS = 4


def step(*args):
    queries, keys, q_gain, tokens, route, gate_weight = (args[i] for i in (0, 1, 3, 6, 8, 10))
    ep, tp = lax.axis_size("ep"), lax.axis_size("tp")
    cap = 2 * tokens.shape[0] * route.shape[1] // ep
    fits = (
        tp == 4
        and ep == 8
        and queries.shape[1] % (2 * q_gain.shape[0]) == 0
        and ep % GROUPS == 0
        and cap % 16 == 0
        and keys.shape[1] == q_gain.shape[0]
        and gate_weight.shape[2] % 128 == 0
        and queries.shape[0] % (16 * tp) == 0
    )
    return local_fused(*args) if fits else local(*args)


def solution(mesh):
    placed = (
        P("ep", "tp"),
        P("ep", "tp"),
        P("ep", "tp"),
        P(),
        P(),
        P("tp", None),
        P(("ep", "tp"), None),
        P(),
        P(("ep", "tp"), None),
        P(("ep", "tp"), None),
        P("ep", None, "tp"),
        P("ep", None, "tp"),
        P("ep", "tp", None),
    )
    return jax.shard_map(
        step,
        mesh=mesh,
        in_specs=placed,
        out_specs=(P(("ep", "tp"), None), P(("ep", "tp"), None)),
        check_vma=False,
    )
```

```python
import functools
import math

import jax
import jax.numpy as jnp
from jax import lax
from jax.experimental import pallas as pl
from jax.experimental.pallas import tpu as pltpu
from jax.sharding import PartitionSpec as P

GRID_W = 64


EPS = 1e-06
THETA = 10000.0


def head_norm(vals, gain):
    vals = vals.astype(jnp.float32)
    return vals * lax.rsqrt(jnp.mean(vals * vals, axis=-1, keepdims=True) + EPS) * gain


def rotate(vals, positions):
    pairs = vals.shape[-1] // 2
    quarter = pairs // 2
    freqs = THETA ** (-jnp.arange(quarter, dtype=jnp.float32) / quarter)
    grid_row = (positions // GRID_W).astype(jnp.float32)
    grid_col = (positions % GRID_W).astype(jnp.float32)
    angle = jnp.concatenate([grid_row[:, None] * freqs, grid_col[:, None] * freqs], axis=-1)
    cosine = jnp.cos(angle)[:, None, :]
    sine = jnp.sin(angle)[:, None, :]
    split = vals.reshape(vals.shape[:-1] + (pairs, 2))
    first = split[..., 0]
    second = split[..., 1]
    turned = jnp.stack([first * cosine - second * sine, first * sine + second * cosine], axis=-1)
    return turned.reshape(vals.shape)


def local(
    queries,
    keys,
    values,
    q_gain,
    k_gain,
    out_weight,
    tokens,
    ffn_gain,
    route,
    route_weight,
    gate_weight,
    up_weight,
    down_weight,
):
    local_rows = queries.shape[0]
    head_size = q_gain.shape[0]
    query_heads = queries.shape[1] // head_size
    key_heads = keys.shape[1] // head_size
    group = query_heads // key_heads
    key_width = key_heads * head_size
    positions = lax.axis_index("ep") * local_rows + jnp.arange(local_rows, dtype=jnp.int32)
    rot_q = rotate(
        head_norm(queries.reshape(local_rows, query_heads, head_size), q_gain), positions
    ).astype(jnp.bfloat16)
    rot_q = rot_q.reshape(local_rows, key_heads, group, head_size)
    rot_k = rotate(
        head_norm(keys.reshape(local_rows, key_heads, head_size), k_gain), positions
    ).astype(jnp.bfloat16)
    joined = jnp.concatenate([rot_k.reshape(local_rows, key_width), values], axis=1)
    scale = head_size ** (-0.5)

    def fold_block(carry, block):
        highest, denom, numer = carry
        key_block = block[:, :key_width].reshape(-1, key_heads, head_size)
        value_block = block[:, key_width:].reshape(-1, key_heads, head_size)
        scores = (
            jnp.einsum("qkgd,skd->qkgs", rot_q, key_block, preferred_element_type=jnp.float32)
            * scale
        )
        new_high = jnp.maximum(highest, jnp.max(scores, axis=-1))
        shrink = jnp.exp(highest - new_high)
        expo = jnp.exp(scores - new_high[..., None])
        denom = denom * shrink + jnp.sum(expo, axis=-1)
        numer = numer * shrink[..., None] + jnp.einsum(
            "qkgs,skd->qkgd",
            expo.astype(jnp.bfloat16),
            value_block,
            preferred_element_type=jnp.float32,
        )
        return ((new_high, denom, numer), None)

    start_high = jnp.full((local_rows, key_heads, group), -1e30, jnp.float32)
    start_denom = jnp.zeros((local_rows, key_heads, group), jnp.float32)
    start_numer = jnp.zeros((local_rows, key_heads, group, head_size), jnp.float32)
    carry = (start_high, start_denom, start_numer)
    piece = lax.all_gather(joined, "ep", axis=0, tiled=True)
    length = piece.shape[0]
    size = length
    while size > 2048 and size % 2 == 0:
        size = size // 2
    blocks = piece.reshape(length // size, size, piece.shape[1])
    carry, _ = lax.scan(fold_block, carry, blocks)
    highest, denom, numer = carry
    attended = (
        (numer / denom[..., None]).astype(jnp.bfloat16).reshape(local_rows, query_heads * head_size)
    )
    own_rows = tokens.shape[0]
    width = tokens.shape[1]
    picks_row = route.shape[1]
    experts = lax.axis_size("ep")
    capacity = 2 * own_rows * picks_row // experts
    token_float = tokens.astype(jnp.float32)
    normed = (
        token_float
        * lax.rsqrt(jnp.mean(token_float * token_float, axis=-1, keepdims=True) + EPS)
        * ffn_gain
    ).astype(jnp.bfloat16)
    flat_route = route.reshape(-1)
    expert_hot = (flat_route[:, None] == jnp.arange(experts, dtype=jnp.int32)[None, :]).astype(
        jnp.int32
    )
    earlier = jnp.cumsum(expert_hot, axis=0) - expert_hot
    rank = jnp.sum(earlier * expert_hot, axis=1)
    slot = flat_route * capacity + rank
    pick_hot = (slot[:, None] == jnp.arange(experts * capacity, dtype=jnp.int32)[None, :]).astype(
        jnp.bfloat16
    )
    row_hot = jnp.sum(pick_hot.reshape(own_rows, picks_row, experts * capacity), axis=1)
    outgoing = jnp.einsum("rs,rd->sd", row_hot, normed, preferred_element_type=jnp.float32).astype(
        jnp.bfloat16
    )
    outgoing = outgoing.reshape(experts, capacity, width)
    gate_local = gate_weight[0]
    up_local = up_weight[0]
    down_local = down_weight[0]
    arrived = lax.all_to_all(outgoing, "ep", split_axis=0, concat_axis=0, tiled=True)
    sources = arrived.shape[0]
    items = arrived.shape[1]
    slot_rows = arrived.reshape(sources * items, width)
    piece = lax.all_gather(slot_rows, "tp", axis=0, tiled=True)
    gate = jnp.dot(piece, gate_local, preferred_element_type=jnp.float32)
    upper = jnp.dot(piece, up_local, preferred_element_type=jnp.float32)
    hidden = (jax.nn.silu(gate) * upper).astype(jnp.bfloat16)
    worked = jnp.dot(hidden, down_local, preferred_element_type=jnp.float32).reshape(
        -1, items, width
    )
    head_partial = jnp.dot(attended, out_weight, preferred_element_type=jnp.float32)
    mixer_sum, expert_sum = (
        lax.psum_scatter(
            head_partial.astype(jnp.bfloat16), "tp", scatter_dimension=0, tiled=True
        ).astype(jnp.float32),
        lax.psum_scatter(worked.astype(jnp.bfloat16), "tp", scatter_dimension=0, tiled=True).astype(
            jnp.float32
        ),
    )
    mixer_out = mixer_sum.astype(jnp.bfloat16)
    home = expert_sum.astype(jnp.bfloat16)
    back = lax.all_to_all(home, "ep", split_axis=0, concat_axis=0, tiled=True)
    copies = jnp.dot(
        pick_hot, back.reshape(experts * capacity, width), preferred_element_type=jnp.float32
    )
    weighted = route_weight[..., None] * copies.reshape(own_rows, picks_row, width)
    mixed = jnp.sum(weighted, axis=1).astype(jnp.bfloat16)
    return (mixer_out, mixed)


def norm_rotate(vals, gain, cosine, sine):
    vals = vals * lax.rsqrt(jnp.mean(vals * vals, axis=-1, keepdims=True) + EPS) * gain
    size = vals.shape[-1]
    lane = lax.broadcasted_iota(jnp.int32, vals.shape, 1)
    up = jnp.concatenate([vals[:, 1:], vals[:, :1]], axis=1)
    down = jnp.concatenate([vals[:, size - 1 :], vals[:, : size - 1]], axis=1)
    swapped = jnp.where(lane % 2 == 0, up, down)
    return vals * cosine + swapped * sine


def fused_kernel(
    dims,
    q_hbm,
    k_hbm,
    v_hbm,
    qg_hbm,
    kg_hbm,
    tok_hbm,
    fg_hbm,
    route_hbm,
    rw_hbm,
    gate_hbm,
    up_hbm,
    down_hbm,
    ow_hbm,
    mix_ref,
    out_ref,
    q_ref,
    k_ref,
    v_ref,
    qg_ref,
    kg_ref,
    tok_ref,
    fg_ref,
    route_t_ref,
    rw_ref,
    wgu,
    wd,
    wo,
    og,
    slots,
    hidden,
    part,
    rs1,
    half,
    rs2,
    home,
    back,
    kvs,
    qp,
    att,
    mpart,
    mrs1,
    mhalf,
    mrs2,
    passing,
    in_sem,
    w_sem,
    a2a_s,
    a2a_r,
    f1_s,
    f1_r,
    f2_s,
    f2_r,
    f3_s,
    f3_r,
    kva_s,
    kva_r,
    kvb_s,
    kvb_r,
    r1_s,
    r1_r,
    r2_s,
    r2_r,
    bk_s,
    bk_r,
    m1_s,
    m1_r,
    m2_s,
    m2_r,
    y2_s,
    y2_r,
):
    ep, tp, cap, groups, tile = dims
    f32, bf16 = jnp.float32, jnp.bfloat16
    per = ep // groups
    order = peer_order(ep)
    place = {mask: i for i, mask in enumerate(order)}
    e = lax.axis_index("ep")
    t = lax.axis_index("tp")
    t1 = t + 1 - 2 * (t % 2)
    t2 = (t + 2) % tp
    own_rows, width = tok_ref.shape
    head_size, rows = k_ref.shape
    heads = q_ref.shape[1] // head_size
    units = hidden.shape[1]
    lane_tile = wgu.shape[2] // 2
    half_ep = ep // 2

    def peer(mask):
        other, bit = e, 1
        while bit < ep:
            if mask & bit:
                other = other + bit * (1 - 2 * ((e // bit) % 2))
            bit *= 2
        return other

    def remote(src, dst, ssem, rsem, pe, pt):
        return pltpu.make_async_remote_copy(
            src_ref=src,
            dst_ref=dst,
            send_sem=ssem,
            recv_sem=rsem,
            device_id={"ep": pe, "tp": pt},
            device_id_type=pl.DeviceIdType.MESH,
        )

    def landed(ref, sem):
        pltpu.make_async_copy(ref, ref, sem).wait()

    barrier = pltpu.get_barrier_semaphore()
    peers = [(peer(mask), t) for mask in range(1, ep)] + [(e, t1), (e, t2)]
    for pe, pt in peers:
        pl.semaphore_signal(
            barrier, inc=1, device_id={"ep": pe, "tp": pt}, device_id_type=pl.DeviceIdType.MESH
        )

    routed = [
        pltpu.make_async_copy(source, target, in_sem.at[n])
        for n, (source, target) in enumerate(
            (
                (route_hbm, route_t_ref),
                (tok_hbm, tok_ref),
                (fg_hbm, fg_ref),
                (rw_hbm, rw_ref),
            )
        )
    ]
    attended = [
        pltpu.make_async_copy(source, target, in_sem.at[len(routed) + n])
        for n, (source, target) in enumerate(
            (
                (k_hbm, k_ref),
                (v_hbm, v_ref),
                (kg_hbm, kg_ref),
                (qg_hbm, qg_ref),
                (q_hbm, q_ref),
            )
        )
    ]
    for copy in routed + attended:
        copy.start()
    for copy in routed + attended:
        copy.wait()
    for n in range(units // lane_tile):
        cols = pl.ds(n * lane_tile, lane_tile)
        for side, source in ((0, gate_hbm), (lane_tile, up_hbm)):
            pltpu.make_async_copy(
                source.at[0, :, cols], wgu.at[n, :, pl.ds(side, lane_tile)], w_sem.at[0]
            ).start()
    load_down = pltpu.make_async_copy(down_hbm.at[0], wd, w_sem.at[1])
    load_out = pltpu.make_async_copy(ow_hbm, wo, w_sem.at[2])
    load_down.start()
    load_out.start()

    slot_rows = ep * cap
    later = lax.broadcasted_iota(jnp.int32, (own_rows, own_rows), 0)
    early = lax.broadcasted_iota(jnp.int32, (own_rows, own_rows), 1)
    picks = []
    sends = jnp.zeros((slot_rows, own_rows), f32)
    topk = route_t_ref.shape[0]
    diag = later == early

    def column(row):
        return jnp.sum(jnp.where(diag, row, jnp.zeros_like(row)), axis=1, keepdims=True)

    def position_of(expert):
        spot = jnp.zeros_like(expert)
        for mask in range(ep):
            spot += jnp.where(expert == peer(mask), place[mask], 0)
        return spot

    mix_weights = [column(rw_ref[k : k + 1, :]) for k in range(topk)]
    columns = [column(route_t_ref[k : k + 1, :]) for k in range(topk)]
    for k in range(topk):
        col = columns[k]
        row = route_t_ref[k : k + 1, :]
        rank_col = jnp.zeros((own_rows, 1), f32)
        rank_row = jnp.zeros((1, own_rows), f32)
        for other in range(topk):
            same = (col == route_t_ref[other : other + 1, :]) & (early < later)
            rank_col += jnp.sum(jnp.where(same, 1.0, 0.0), axis=1, keepdims=True)
            same_t = (columns[other] == row) & (later < early)
            rank_row += jnp.sum(jnp.where(same_t, 1.0, 0.0), axis=0, keepdims=True)
        slot_col = (position_of(col) * cap).astype(f32) + rank_col
        slot_row = (position_of(row) * cap).astype(f32) + rank_row
        lanes = lax.broadcasted_iota(jnp.int32, (own_rows, slot_rows), 1).astype(f32)
        picks.append(jnp.where(lanes == slot_col, 1.0, 0.0).astype(bf16))
        subs = lax.broadcasted_iota(jnp.int32, (slot_rows, own_rows), 0).astype(f32)
        sends += jnp.where(subs == slot_row, 1.0, 0.0)
    tok = tok_ref[...].astype(f32)
    normed = (
        tok * lax.rsqrt(jnp.mean(tok * tok, axis=-1, keepdims=True) + EPS) * fg_ref[...]
    ).astype(bf16)
    outgoing = (
        jnp.dot(sends.astype(bf16), normed, preferred_element_type=f32)
        .astype(bf16)
        .reshape(ep, cap, width)
    )
    og[...] = outgoing
    slots[place[0] // per, 0, place[0] % per] = outgoing[place[0]]

    with jax.named_scope("barrier"):
        pl.semaphore_wait(barrier, len(peers))

    a2a, f1, f2, f3, y2 = {}, {}, {}, {}, {}
    for i in range(ep):
        g, m = i // per, i % per
        if order[i]:
            a2a[i] = remote(
                og.at[i], slots.at[g, 0, m], a2a_s, a2a_r.at[i], peer(order[i]), t
            )
        f1[i] = remote(slots.at[g, 0, m], slots.at[g, 1, m], f1_s, f1_r.at[g], e, t1)
        mask = order[i]
        if 0 < mask < half_ep:
            f2[i] = remote(og.at[i], passing.at[mask], f2_s, f2_r.at[i], e, t2)
            y2[i] = remote(
                passing.at[mask], slots.at[g, 2, m], y2_s, y2_r.at[mask], peer(mask), t
            )
        else:
            f2[i] = remote(slots.at[g, 0, m], slots.at[g, 2, m], f2_s, f2_r.at[i], e, t2)
        f3[i] = remote(slots.at[g, 2, m], slots.at[g, 3, m], f3_s, f3_r.at[g], e, t1)
    kva, kvb = {}, {}
    for k in range(half_ep):
        kvb[k] = remote(kvs.at[0, k], kvs.at[1, k], kvb_s, kvb_r, peer(1), t)
        if k in (1, 2):
            kva[k] = remote(
                kvs.at[0, 0], kvs.at[0, k], kva_s, kva_r.at[k], peer(2 * k), t
            )
        if k == 3:
            kva[k] = remote(
                kvs.at[0, 2], kvs.at[0, 3], kva_s, kva_r.at[k], peer(2), t
            )

    near, far = issue_order(ep)
    for mask in near:
        a2a[place[mask]].start()
    for mask in range(1, half_ep):
        f2[place[mask]].start()
    for mask in far:
        a2a[place[mask]].start()

    def forward(mask):
        i = place[mask]
        with jax.named_scope(f"fwd{mask}"):
            if mask:
                a2a[i].wait_recv()
            if not 0 < mask < half_ep:
                f2[i].start()
            f1[i].start()

    def pass_on(mask):
        i = place[mask]
        with jax.named_scope(f"pass{mask}"):
            f2[i].wait_recv()
            y2[i].start()

    def relay(mask):
        i = place[mask]
        with jax.named_scope(f"relay{mask}"):
            (y2[i] if 0 < mask < half_ep else f2[i]).wait_recv()
            f3[i].start()

    forward(0)

    position = e * rows + lax.broadcasted_iota(jnp.int32, (rows, head_size), 0)
    channel = lax.broadcasted_iota(jnp.int32, (rows, head_size), 1)
    quarter = head_size // 4
    power = (channel // 2) % quarter
    freq = jnp.exp(power.astype(f32) * (-math.log(THETA) / quarter))
    grid_row = position // GRID_W
    spot = jnp.where(channel < head_size // 2, grid_row, position - grid_row * GRID_W)
    angle = spot.astype(f32) * freq
    cosine = jnp.cos(angle)
    sine = jnp.sin(angle) * jnp.where(channel % 2 == 0, -1.0, 1.0)
    both = jnp.concatenate([k_ref[...], v_ref[...]], axis=0).astype(f32).T
    rot_k = norm_rotate(both[:, :head_size], kg_ref[...], cosine, sine)
    kvs[0, 0, :, pl.ds(0, head_size)] = rot_k.astype(bf16)
    kvs[0, 0, :, pl.ds(head_size, head_size)] = both[:, head_size:].astype(bf16)

    kvb[0].start()

    for h in range(heads):
        lanes = pl.ds(h * head_size, head_size)
        turned = norm_rotate(q_ref[:, lanes].astype(f32), qg_ref[...], cosine, sine)
        qp[h, :, pl.ds(0, head_size)] = turned.astype(bf16)
        qp[h, :, pl.ds(head_size, head_size)] = jnp.zeros((rows, head_size), bf16)

    def share_keys(k):
        with jax.named_scope(f"share{k}"):
            kva[k].wait_recv()
            if k == 2:
                kva[3].start()
            kvb[k].start()

    scale = head_size ** (-0.5) * math.log2(math.e)
    half_rows = rows // 2
    y = t // 2
    stack = 2

    def attend(side, h):
        start = pl.multiple_of(side * half_rows, half_rows)
        joined = kvs[...].reshape(ep * rows, 2 * head_size)
        chosen = qp[pl.ds(h, stack), pl.ds(start, half_rows), :]
        scores = lax.dot_general(
            chosen.reshape(stack * half_rows, 2 * head_size),
            joined,
            (((1,), (1,)), ((), ())),
            preferred_element_type=f32,
        )
        expo = jnp.exp2((scores - jnp.max(scores, axis=-1, keepdims=True)) * scale)
        denom = jnp.sum(expo, axis=-1, keepdims=True)
        numer = jnp.dot(expo.astype(bf16), joined, preferred_element_type=f32)
        result = (numer[:, head_size:] / denom).astype(bf16)
        for k in range(stack):
            att[pl.ds(start, half_rows), pl.ds((h + k) * head_size, head_size)] = result[
                k * half_rows : (k + 1) * half_rows
            ]

    mrows = rows // tp
    homes = [t, t1, t2, (t1 + 2) % tp]
    m1 = [
        remote(mpart.at[2 * i + 1], mrs1.at[i], m1_s, m1_r.at[i], e, t1) for i in range(2)
    ]
    m2 = remote(mhalf, mrs2, m2_s, m2_r, e, t2)

    def project(js):
        for j in js:
            piece = att[pl.ds(pl.multiple_of(homes[j] * mrows, mrows), mrows), :]
            mpart[j] = jnp.dot(piece, wo[...], preferred_element_type=f32).astype(bf16)
            if j % 2:
                m1[j // 2].start()

    def feed_wait(g):
        with jax.named_scope(f"feedwait{g}"):
            landed(slots.at[g, 1], f1_r.at[g])
            landed(slots.at[g, 3], f3_r.at[g])

    rows_g = tp * per * cap

    def up(g):
        with jax.named_scope(f"up{g}"):
            chosen = slots[g].reshape(rows_g, width)
            for n in range(units // lane_tile):
                both = jnp.dot(chosen, wgu[n], preferred_element_type=f32)
                gate = both[:, :lane_tile]
                act = gate / (1.0 + jnp.exp(-gate)) * both[:, lane_tile:]
                hidden[:, pl.ds(n * lane_tile, lane_tile)] = act.astype(bf16)

    def down(g):
        with jax.named_scope(f"down{g}"):
            for n in range(width // tile):
                cols = pl.ds(n * tile, tile)
                result = jnp.dot(hidden[...], wd[:, cols], preferred_element_type=f32)
                part[g, :, :, :, cols] = result.astype(bf16).reshape(tp, per, cap, tile)
        r1[g, 1].start()
        r1[g, 0].start()

    r1, r2 = {}, {}
    for g in range(groups):
        for i in range(2):
            r1[g, i] = remote(
                part.at[g, 2 * i + 1], rs1.at[g, i], r1_s, r1_r.at[g, i], e, t1
            )
        r2[g] = remote(half.at[g], rs2.at[g], r2_s, r2_r.at[g], e, t2)
    bk = {}
    for i in range(ep):
        if order[i]:
            bk[i] = remote(
                home.at[i // per, i % per], back.at[i], bk_s, bk_r, peer(order[i]), t
            )

    def pair_sum(g):
        with jax.named_scope(f"pairsum{g}"):
            r1[g, 1].wait_recv()
            half[g] = (part[g, 2].astype(f32) + rs1[g, 1].astype(f32)).astype(bf16)
            r2[g].start()

    def finish(g):
        with jax.named_scope(f"finish{g}"):
            r1[g, 0].wait_recv()
            r2[g].wait_recv()
            total = (
                part[g, 0].astype(f32) + rs1[g, 0].astype(f32) + rs2[g].astype(f32)
            ).astype(bf16)
            home[g] = total
            for i in range(g * per, (g + 1) * per):
                if order[i]:
                    bk[i].start()
                else:
                    back[i] = total[i % per]

    def mixer_half():
        with jax.named_scope("mixhalf"):
            m1[1].wait_recv()
            mhalf[...] = (mpart[2].astype(f32) + mrs1[1].astype(f32)).astype(bf16)
            m2.start()

    kva[2].start()
    pass_on(1)
    forward(1)
    pass_on(2)
    pass_on(3)
    kva[1].start()
    relay(1)
    forward(4)
    forward(2)
    forward(3)
    relay(0)
    pltpu.make_async_copy(wgu, wgu, w_sem.at[0]).wait()
    load_down.wait()
    relay(4)
    forward(5)
    feed_wait(0)
    up(0)
    relay(2)
    forward(6)
    down(0)
    forward(7)
    relay(5)
    feed_wait(1)
    pair_sum(0)
    share_keys(2)
    up(1)
    relay(3)
    relay(6)
    down(1)
    relay(7)
    share_keys(1)
    feed_wait(2)
    up(2)
    share_keys(3)
    pair_sum(1)
    down(2)
    feed_wait(3)
    up(3)
    finish(0)
    pair_sum(2)
    down(3)
    with jax.named_scope("kvwait"):
        landed(kvs.at[1], kvb_r)
    with jax.named_scope("att0"):
        attend(1 - y, 0)
    pair_sum(3)
    finish(1)
    with jax.named_scope("att1"):
        attend(1 - y, 2)
    load_out.wait()
    with jax.named_scope("project"):
        project((3, 2))
    with jax.named_scope("att2"):
        attend(y, 0)
    mixer_half()
    finish(2)
    with jax.named_scope("att3"):
        attend(y, 2)
    with jax.named_scope("project"):
        project((1, 0))
    finish(3)
    others = pl.ds(0, ep - 1)
    landed(og.at[others], a2a_s)
    for sem in (f1_s, f2_s, f3_s):
        landed(og, sem)
    landed(og.at[pl.ds(0, half_ep - 1)], y2_s)
    landed(kvs.at[0, pl.ds(0, half_ep - 1)], kva_s)
    landed(kvs.at[0], kvb_s)
    landed(rs1, r1_s)
    landed(rs2, r2_s)
    with jax.named_scope("bkwait"):
        landed(back.at[pl.ds(0, ep - 1)], bk_r)
    returned = back[...].reshape(slot_rows, width)
    chosen = jnp.dot(jnp.concatenate(picks, axis=0), returned, preferred_element_type=f32)
    mixed = jnp.zeros((own_rows, width), f32)
    for k in range(topk):
        mixed += mix_weights[k] * chosen[k * own_rows : (k + 1) * own_rows]
    out_ref[...] = mixed.astype(bf16)
    with jax.named_scope("mwait"):
        m1[0].wait_recv()
        m2.wait_recv()
    mix_ref[...] = (
        mpart[0].astype(f32) + mrs1[0].astype(f32) + mrs2[...].astype(f32)
    ).astype(bf16)
    landed(og.at[others], bk_s)
    landed(mrs1, m1_s)
    m2.wait_send()


def peer_order(ep):
    half = ep // 2
    near = tuple(range(1, half)) + (0,)
    return tuple(m for i, k in enumerate(near) for m in (k, half + i))


def issue_order(ep):
    return (1, 2, 3), tuple(range(4, ep))


def store_kernel(mix_ref, rows_ref, mix_out, rows_out, sems):
    copies = [
        pltpu.make_async_copy(mix_ref, mix_out, sems.at[0]),
        pltpu.make_async_copy(rows_ref, rows_out, sems.at[1]),
    ]
    for copy in copies:
        copy.start()
    for copy in copies:
        copy.wait()


def local_fused(
    queries,
    keys,
    values,
    q_gain,
    k_gain,
    out_weight,
    tokens,
    ffn_gain,
    route,
    route_weight,
    gate_weight,
    up_weight,
    down_weight,
):
    ep = lax.axis_size("ep")
    tp = lax.axis_size("tp")
    rows = queries.shape[0]
    head_size = q_gain.shape[0]
    heads = queries.shape[1] // head_size
    own_rows, width = tokens.shape
    cap = 2 * own_rows * route.shape[1] // ep
    units = gate_weight.shape[2]
    lane_tile = 128
    tile = math.gcd(width, 1024)
    groups = GROUPS
    per = ep // groups
    bf16 = jnp.bfloat16
    vmem = pl.BlockSpec(memory_space=pltpu.VMEM)
    hbm = pl.BlockSpec(memory_space=pl.ANY)
    dma = pltpu.SemaphoreType.DMA
    mrows = rows // tp
    flops = 2 * tp * ep * cap * width * units * 3 + 4 * heads * rows * rows * ep * head_size
    loaded = (
        queries,
        keys.T,
        values.T,
        q_gain[None, :],
        k_gain[None, :],
        tokens,
        ffn_gain[None, :],
        route.T,
        route_weight.T,
    )
    held = pl.pallas_call(
        functools.partial(fused_kernel, (ep, tp, cap, groups, tile)),
        out_shape=(
            pltpu.VMEM((mrows, width), bf16),
            pltpu.VMEM((own_rows, width), bf16),
        ),
        in_specs=[hbm] * 13,
        out_specs=(vmem, vmem),
        scratch_shapes=[pltpu.VMEM(part.shape, part.dtype) for part in loaded]
        + [
            pltpu.VMEM((units // lane_tile, width, 2 * lane_tile), bf16),
            pltpu.VMEM((units, width), bf16),
            pltpu.VMEM(out_weight.shape, bf16),
            pltpu.VMEM((ep, cap, width), bf16),
            pltpu.VMEM((groups, tp, per, cap, width), bf16),
            pltpu.VMEM((tp * per * cap, units), bf16),
            pltpu.VMEM((groups, tp, per, cap, width), bf16),
            pltpu.VMEM((groups, 2, per, cap, width), bf16),
            pltpu.VMEM((groups, per, cap, width), bf16),
            pltpu.VMEM((groups, per, cap, width), bf16),
            pltpu.VMEM((groups, per, cap, width), bf16),
            pltpu.VMEM((ep, cap, width), bf16),
            pltpu.VMEM((2, ep // 2, rows, 2 * head_size), bf16),
            pltpu.VMEM((heads, rows, 2 * head_size), bf16),
            pltpu.VMEM((rows, heads * head_size), bf16),
            pltpu.VMEM((tp, mrows, width), bf16),
            pltpu.VMEM((2, mrows, width), bf16),
            pltpu.VMEM((mrows, width), bf16),
            pltpu.VMEM((mrows, width), bf16),
            pltpu.VMEM((ep // 2, cap, width), bf16),
            dma((len(loaded),)),
            dma((3,)),
        ]
        + [dma, dma((ep,)), dma, dma((groups,)), dma, dma((ep,)), dma, dma((groups,))]
        + [dma, dma((ep // 2,)), dma, dma]
        + [dma, dma((groups, 2)), dma, dma((groups,)), dma, dma]
        + [dma, dma((2,)), dma, dma]
        + [dma, dma((ep // 2,))],
        compiler_params=pltpu.CompilerParams(
            collective_id=0, has_side_effects=True, vmem_limit_bytes=60 * 1024 * 1024
        ),
        cost_estimate=pl.CostEstimate(
            flops=flops, bytes_accessed=3 * 2 * width * units, transcendentals=0
        ),
    )(
        *loaded,
        gate_weight,
        up_weight,
        down_weight,
        out_weight,
    )
    return pl.pallas_call(
        store_kernel,
        out_shape=tuple(jax.ShapeDtypeStruct(part.shape, bf16) for part in held),
        in_specs=[vmem] * len(held),
        out_specs=(hbm,) * len(held),
        scratch_shapes=[dma((len(held),))],
    )(*[pltpu.with_memory_space_constraint(part, pltpu.VMEM) for part in held])


GROUPS = 4


def step(*args):
    queries, keys, q_gain, tokens, route, gate_weight = (args[i] for i in (0, 1, 3, 6, 8, 10))
    ep, tp = lax.axis_size("ep"), lax.axis_size("tp")
    cap = 2 * tokens.shape[0] * route.shape[1] // ep
    fits = (
        tp == 4
        and ep == 8
        and queries.shape[1] % (2 * q_gain.shape[0]) == 0
        and ep % GROUPS == 0
        and cap % 16 == 0
        and keys.shape[1] == q_gain.shape[0]
        and gate_weight.shape[2] % 128 == 0
        and queries.shape[0] % (16 * tp) == 0
    )
    return local_fused(*args) if fits else local(*args)


def solution(mesh):
    placed = (
        P("ep", "tp"),
        P("ep", "tp"),
        P("ep", "tp"),
        P(),
        P(),
        P("tp", None),
        P(("ep", "tp"), None),
        P(),
        P(("ep", "tp"), None),
        P(("ep", "tp"), None),
        P("ep", None, "tp"),
        P("ep", None, "tp"),
        P("ep", "tp", None),
    )
    return jax.shard_map(
        step,
        mesh=mesh,
        in_specs=placed,
        out_specs=(P(("ep", "tp"), None), P(("ep", "tp"), None)),
        check_vma=False,
    )
```
